128 devices in a mesh: ep: 16 (over z, x), tp: 8 (over y, core).
Axes of the slice: x: 4, y: 4, z: 4, core: 2. Of those that a mesh axis runs over, the one named last changes fastest.
Arguments:
- queries: bfloat16 [32768, 512], P('ep', 'tp'), may hold values from -6 to 6
- head_key_rows: bfloat16 [32768, 512], P('ep', 'tp'), may hold values from -6 to 6
- head_value_rows: bfloat16 [32768, 1024], P('ep', 'tp'), may hold values from -18 to 18
- log_input_gate: float32 [32768, 8], P('ep', 'tp'), may hold values from -6 to 120
- forget_logits: float32 [32768, 8], P('ep', 'tp'), may hold values from -8 to 8
- head_forget_bias: float32 [8], P('tp'), may hold values from 3 to 20
- extra_log_forget: float32 [32768, 8], P('ep', 'tp'), may hold values from -1 to 0
- output_gate_logits: bfloat16 [32768, 1024], P('ep', 'tp'), may hold values from -6 to 6
- head_norm_gain: float32 [1024], P('tp'), may hold values from 0.1 to 1.9
- mixer_output_weight: bfloat16 [1024, 2048], replicated, may hold values from -0.1875 to 0.1875
- second_batch_input: bfloat16 [24576, 2048], P(('ep', 'tp')), may hold values from -6 to 6
- expert_norm_gain: float32 [2048], replicated, may hold values from 0.1 to 1.9
- routed_expert_index: int32 [24576, 2], P(('ep', 'tp')), may hold values from 0 to 127, all different within a row; in each aligned block of 192 rows (0 to 191, 192 to 383, ...) at most 4 rows name the same one
- routed_copy_weight: float32 [24576, 2], P(('ep', 'tp')), may hold values from 0.3 to 1.5
- routed_gate_weight: bfloat16 [128, 2048, 1024], P(('ep', 'tp')), may hold values from -0.125 to 0.125
- routed_up_weight: bfloat16 [128, 2048, 1024], P(('ep', 'tp')), may hold values from -0.125 to 0.125
- routed_down_weight: bfloat16 [128, 1024, 2048], P(('ep', 'tp')), may hold values from -0.1875 to 0.1875
- shared_gate_weight: bfloat16 [2048, 384], replicated, may hold values from -0.125 to 0.125
- shared_up_weight: bfloat16 [2048, 384], replicated, may hold values from -0.125 to 0.125
- shared_down_weight: bfloat16 [384, 2048], replicated, may hold values from -0.3125 to 0.3125
Outputs:
- mixer_first_output: bfloat16 [32768, 2048], P(('ep', 'tp'))
- moe_out: bfloat16 [24576, 2048], P(('ep', 'tp'))
The draws below stay inside these ranges and needn't reach their ends.
Inputs may be any that keep to these rules, and one draw needn't show every extreme that they name: `routed_expert_index`: in each aligned block of 192 rows (the rows of one device) no expert is named by more than 4 rows, and in some blocks one expert is named by exactly 4; every expert is named somewhere.
All inputs are finite; a program needn't handle non-finite values.
Results may differ from the reference program's by a relative error of at most 0.0068.
Values may be sent and summed in bfloat16 or wider, within the bound.
No kernel may reach another device: no remote copies, remote signals or barrier semaphores. Data moves between devices by JAX's collectives and lax.ppermute only.
A program may use at most 128 MiB of HBM per device.

```python
import math
from functools import partial
import jax
import jax.numpy as jnp
import numpy as np
from jax import lax

D = 2048
HEADS = 8
DK = 64
DV = 128
BLK = 128
TOPK = 2
FE = 1024
FS = 384
MOE_DEV = 192
EXPERTS = 128
TOK1 = 32768
TOK2 = 24576
CAP = 4


def draw_head_value_rows(key, part):
    key_base = jax.random.fold_in(key, 15)
    head_of_column = jnp.arange(HEADS * DV, dtype=jnp.int32) // DV
    fraction = head_of_column.astype(jnp.float32) / (HEADS - 1)
    base = jnp.clip(jax.random.normal(key_base, (TOK1, HEADS * DV), jnp.float32), -6.0, 6.0)
    column_scale = jnp.exp(fraction * jnp.log(3.0))
    return (base * column_scale[None, :]).astype(jnp.bfloat16)


def draw_head_forget_bias(key, part):
    key_order, key_slow, key_fast = jax.random.split(jax.random.fold_in(key, 11), 3)
    slow_count = HEADS // 2
    ranking = jax.random.permutation(key_order, HEADS)
    is_slow = ranking < slow_count
    slow_rate = jnp.exp(jax.random.uniform(key_slow, (HEADS,), jnp.float32, jnp.log(0.3), jnp.log(1.0))) / TOK1
    fast_rate = jnp.exp(jax.random.uniform(key_fast, (HEADS,), jnp.float32, jnp.log(1.0 / 100.0), jnp.log(1.0 / 30.0)))
    return -jnp.log(jnp.where(is_slow, slow_rate, fast_rate)).astype(jnp.float32)


def draw_forget_logits(key, part):
    key_base, key_offset = jax.random.split(jax.random.fold_in(key, 12), 2)
    base = jnp.clip(jax.random.normal(key_base, (TOK1, HEADS), jnp.float32), -6.0, 6.0)
    offsets = jax.random.uniform(key_offset, (64, HEADS), jnp.float32, -0.7, 0.7)
    return (base + jnp.repeat(offsets, TOK1 // 64, axis=0)).astype(jnp.float32)


def draw_extra_log_forget(key, part):
    key_place, key_value = jax.random.split(jax.random.fold_in(key, 13), 2)
    places = jax.random.randint(key_place, (4, HEADS), 0, TOK1)
    values = jnp.log(jax.random.uniform(key_value, (4, HEADS), jnp.float32, 0.5, 0.8))
    columns = jnp.broadcast_to(jnp.arange(HEADS, dtype=jnp.int32)[None, :], (4, HEADS))
    return jnp.zeros((TOK1, HEADS), jnp.float32).at[places, columns].set(values)


def draw_log_input_gate(key, part):
    key_base = jax.random.fold_in(jax.random.fold_in(key, 14), 0)
    return jnp.clip(jax.random.normal(key_base, (TOK1, HEADS), jnp.float32), -6.0, 6.0)


def steps_of(stream_key, extent, pieces, smallest, top_value):
    def one(axis_at, parts):
        steps = jax.random.uniform(jax.random.fold_in(jax.random.fold_in(stream_key, 6), axis_at), (parts,), jnp.float32, smallest / len(pieces), top_value / len(pieces))
        return jnp.repeat(jnp.exp(steps), extent[axis_at] // parts).reshape((-1,) + (1,) * (len(extent) - axis_at - 1))

    loudness = one(*pieces[0])
    for cut in pieces[1:]:
        loudness = loudness * one(*cut)
    return loudness


def assign_block(own_key, own, number, rows, amount, top, limit, lean):
    order = jax.random.permutation(own_key, amount)
    packed, common = load_shares(amount, rows * top, limit, lean, True), load_shares(amount, rows * top, limit, lean, False)
    places = jnp.arange(amount)

    def named(tallies, turn):
        used = int((tallies > 0).sum())
        fixed = max(1, used // 4)
        passed = fixed + (places - fixed + turn * (used - fixed)) % max(1, amount - fixed)
        return jnp.zeros((amount,), jnp.int32).at[order[jnp.where(places < fixed, places, passed)]].set(jnp.asarray(tallies, jnp.int32))

    tallies = jnp.where(number % 4 == 0, named(packed, number // 4), named(common, number - number // 4 - 1))
    mixed = jax.random.permutation(jax.random.fold_in(own, 3), amount)
    giver, sink = mixed[0:amount // 2 * 2:2], mixed[1:amount // 2 * 2:2]
    margin = jnp.minimum(tallies[giver] - 1, limit - tallies[sink]) // 2
    margin = jnp.where((giver == order[0]) | (sink == order[0]) | (tallies[sink] == 0), 0, jnp.maximum(margin, 0))
    passed = jax.random.randint(jax.random.fold_in(own, 4), (amount // 2,), 0, 1 << 20) % (margin + 1)
    tallies = tallies.at[giver].add(-passed).at[sink].add(passed)
    labels = jnp.searchsorted(jnp.cumsum(tallies), jnp.arange(rows * top), side="right").astype(jnp.int32)
    table = labels.reshape(top, rows).T
    table = table[jax.random.permutation(jax.random.fold_in(own, 1), rows)]
    turn = jax.random.randint(jax.random.fold_in(own, 2), (rows, 1), 0, top)
    return jnp.take_along_axis(table, (jnp.arange(top)[None, :] + turn) % top, axis=1)


def load_shares(amount, total, reach, lean, full):
    loads = [(1 << 20) // math.isqrt(grade ** lean) + 1 for grade in range(1, amount + 1)]
    largest = reach if full else min(reach, max(-(-total // amount), total * loads[0] // sum(loads)))
    least = 1 if total - largest >= amount - 1 else 0
    given, spare = [largest] + [least] * (amount - 1), total - largest - least * (amount - 1)
    while spare > 0:
        free = [i for i in range(1, amount) if given[i] < largest] or [i for i in range(1, amount) if given[i] < reach]
        mass, left = sum([loads[i] for i in free]), spare
        for i in free:
            addition = min(reach - given[i], max(1, left * loads[i] // mass), spare)
            given[i] = given[i] + addition
            spare = spare - addition
    return np.array(given)


def scatter_about(own_key, shape, width, reach, cuts=(), kind=jnp.bfloat16):
    level = steps_of(own_key, shape, cuts, -0.22, 0.18) if cuts else 1.0
    values = jax.random.normal(own_key, shape, jnp.float32) * width * level
    return jnp.minimum(jnp.maximum(values, -reach), reach).astype(kind)


def setup_inputs(seed: int = 0) -> dict:
    seeds = jax.random.split(jax.random.key(seed), 21)
    queries = scatter_about(seeds[0], (TOK1, HEADS * DK), 1.0, 6.0, ((0, 16), (1, 8)))
    head_key_rows = scatter_about(seeds[1], (TOK1, HEADS * DK), 1.0, 6.0, ((0, 16), (1, 8)))
    head_value_rows = draw_head_value_rows(jax.random.fold_in(seeds[20], 71), 0)
    log_input_gate = draw_log_input_gate(jax.random.fold_in(seeds[20], 71), 0)
    forget_logits = draw_forget_logits(jax.random.fold_in(seeds[20], 71), 0)
    head_forget_bias = draw_head_forget_bias(jax.random.fold_in(seeds[20], 71), 0)
    extra_log_forget = draw_extra_log_forget(jax.random.fold_in(seeds[20], 71), 0)
    output_gate_logits = scatter_about(seeds[7], (TOK1, HEADS * DV), 1.0, 6.0, ((0, 16), (1, 8)))
    head_norm_gain = jnp.clip(1.0 + 0.18 * jax.random.normal(seeds[8], (HEADS * DV,), jnp.float32), 0.1, 1.9)
    mixer_output_weight = scatter_about(seeds[9], (HEADS * DV, D), (HEADS * DV) ** -0.5, 0.1875)
    second_batch_input = scatter_about(seeds[10], (TOK2, D), 1.0, 6.0, ((0, 128),))
    expert_norm_gain = jnp.clip(1.0 + 0.18 * jax.random.normal(seeds[11], (D,), jnp.float32), 0.1, 1.9)
    routed_expert_index_keys = jax.random.split(jax.random.fold_in(seeds[12], 1), TOK2 // MOE_DEV)
    routed_expert_index_turns = jax.random.permutation(jax.random.fold_in(seeds[12], 3), TOK2 // MOE_DEV)
    routed_expert_index = jax.vmap(lambda own, number: assign_block(jax.random.fold_in(seeds[12], 2), own, number, MOE_DEV, EXPERTS, TOPK, CAP, 1))(routed_expert_index_keys, routed_expert_index_turns).reshape((TOK2, TOPK))
    routed_copy_weight = jnp.clip(jnp.exp(math.log(1.5) - 1.60943787 * jax.random.uniform(seeds[13], (TOK2, TOPK), jnp.float32) ** steps_of(seeds[13], (TOK2, TOPK), ((0, 128),), -0.2, 0.2)), 0.3, 1.5)
    routed_gate_weight = scatter_about(seeds[14], (EXPERTS, D, FE), D ** -0.5, 0.125, ((0, 128),))
    routed_up_weight = scatter_about(seeds[15], (EXPERTS, D, FE), D ** -0.5, 0.125, ((0, 128),))
    routed_down_weight = scatter_about(seeds[16], (EXPERTS, FE, D), FE ** -0.5, 0.1875, ((0, 128),))
    shared_gate_weight = scatter_about(seeds[17], (D, FS), D ** -0.5, 0.125)
    shared_up_weight = scatter_about(seeds[18], (D, FS), D ** -0.5, 0.125)
    shared_down_weight = scatter_about(seeds[19], (FS, D), FS ** -0.5, 0.3125)
    return {"queries": queries, "head_key_rows": head_key_rows, "head_value_rows": head_value_rows, "log_input_gate": log_input_gate, "forget_logits": forget_logits, "head_forget_bias": head_forget_bias, "extra_log_forget": extra_log_forget, "output_gate_logits": output_gate_logits, "head_norm_gain": head_norm_gain, "mixer_output_weight": mixer_output_weight, "second_batch_input": second_batch_input, "expert_norm_gain": expert_norm_gain, "routed_expert_index": routed_expert_index, "routed_copy_weight": routed_copy_weight, "routed_gate_weight": routed_gate_weight, "routed_up_weight": routed_up_weight, "routed_down_weight": routed_down_weight, "shared_gate_weight": shared_gate_weight, "shared_up_weight": shared_up_weight, "shared_down_weight": shared_down_weight}


exact_einsum = partial(jnp.einsum, precision=lax.Precision.HIGHEST)

def memory_step(carry, inputs):
    memory, normalizer, running_max = carry
    query_block, key_block, value_block, in_block, forget_block = inputs
    cumulative = jnp.cumsum(forget_block, axis=-1)
    lower = jnp.tril(jnp.ones((BLK, BLK), dtype=bool))
    pair_gap = jnp.where(lower, cumulative[:, :, None] - cumulative[:, None, :] + in_block[:, None, :], -jnp.inf)
    carried = cumulative + running_max[:, None]
    stabilizer = jnp.maximum(carried, lax.optimization_barrier(jnp.max(pair_gap, axis=-1)))
    local_weight = jnp.exp(pair_gap - stabilizer[..., None])
    carry_weight = jnp.exp(carried - stabilizer)
    scores = exact_einsum('htd,hsd->hts', query_block, key_block) * local_weight
    numerator = carry_weight[..., None] * exact_einsum('htd,hde->hte', query_block, memory) + exact_einsum('hts,hse->hte', scores, value_block)
    denominator = carry_weight * exact_einsum('htd,hd->ht', query_block, normalizer) + lax.optimization_barrier(jnp.sum(scores, axis=-1))
    hidden = numerator / jnp.maximum(jnp.abs(denominator), jnp.exp(-stabilizer))[..., None]
    block_total = cumulative[:, -1]
    key_gap = block_total[:, None] - cumulative + in_block
    new_max = jnp.maximum(block_total + running_max, lax.optimization_barrier(jnp.max(key_gap, axis=-1)))
    decay_factor = jnp.exp(block_total + running_max - new_max)
    weighted_keys = jnp.exp(key_gap - new_max[:, None])[..., None] * key_block
    memory = decay_factor[:, None, None] * memory + exact_einsum('hsd,hse->hde', weighted_keys, value_block)
    normalizer = decay_factor[:, None] * normalizer + lax.optimization_barrier(jnp.sum(weighted_keys, axis=1))
    return ((memory, normalizer, new_max), hidden)

def mixer_portion(queries, head_key_rows, head_value_rows, log_input_gate, forget_logits, head_forget_bias, extra_log_forget, output_gate_logits, head_norm_gain, mixer_output_weight):
    positions = queries.shape[0]
    block_count = positions // BLK

    def to_blocks(array, size):
        return array.astype(jnp.float32).reshape(block_count, BLK, HEADS, size).transpose(0, 2, 1, 3)

    def gate_block_list(array):
        return array.reshape(block_count, BLK, HEADS).transpose(0, 2, 1)
    query_blocks = to_blocks(queries, DK) * DK ** (-0.5)
    key_blocks = to_blocks(head_key_rows, DK)
    value_blocks = to_blocks(head_value_rows, DV)
    forget_log_value = jax.nn.log_sigmoid(forget_logits + head_forget_bias[None, :]) + extra_log_forget
    start = (jnp.zeros((HEADS, DK, DV), jnp.float32), jnp.zeros((HEADS, DK), jnp.float32), jnp.zeros((HEADS,), jnp.float32))
    _, hidden = lax.scan(memory_step, start, (query_blocks, key_blocks, value_blocks, gate_block_list(log_input_gate), gate_block_list(forget_log_value)))
    hidden = hidden.transpose(0, 2, 1, 3).reshape(positions, HEADS, DV)
    scaled = hidden * lax.rsqrt(lax.optimization_barrier(jnp.mean(hidden * hidden, axis=(1, 2), keepdims=True)) + 1e-06)
    scaled = scaled * head_norm_gain.reshape(HEADS, DV)
    gated = scaled * jax.nn.sigmoid(output_gate_logits.astype(jnp.float32).reshape(positions, HEADS, DV))
    mixed = gated.reshape(positions, HEADS * DV).astype(jnp.bfloat16)
    return jnp.dot(mixed, mixer_output_weight, preferred_element_type=jnp.float32).astype(jnp.bfloat16)

def expert_part(second_batch_input, expert_norm_gain, routed_expert_index, routed_copy_weight, routed_gate_weight, routed_up_weight, routed_down_weight, shared_gate_weight, shared_up_weight, shared_down_weight):
    token_count = second_batch_input.shape[0]
    floats = second_batch_input.astype(jnp.float32)
    normed = (floats * lax.rsqrt(lax.optimization_barrier(jnp.mean(floats * floats, axis=-1, keepdims=True)) + 1e-06) * expert_norm_gain).astype(jnp.bfloat16)
    block_count = token_count // MOE_DEV
    expert_list = routed_expert_index.reshape(block_count, MOE_DEV * TOPK)
    one_hot = (expert_list[..., None] == jnp.arange(EXPERTS, dtype=jnp.int32)).astype(jnp.int32)
    position = lax.optimization_barrier(jnp.sum((jnp.cumsum(one_hot, axis=1) - one_hot) * one_hot, axis=-1))
    slot_index = expert_list * (block_count * CAP) + jnp.arange(block_count, dtype=jnp.int32)[:, None] * CAP + position
    slot_flat = slot_index.reshape(-1)
    slot_table = jnp.full((EXPERTS * block_count * CAP,), token_count, jnp.int32)
    slot_table = slot_table.at[slot_flat].set(jnp.arange(token_count * TOPK, dtype=jnp.int32) // TOPK)
    padded = jnp.concatenate([normed, jnp.zeros((1, D), jnp.bfloat16)], axis=0)

    def one_expert(operands):
        table_row, gate_weight, up_weight, down_weight = operands
        row_block = padded[table_row]
        gate_vals = jnp.dot(row_block, gate_weight, preferred_element_type=jnp.float32)
        up_vals = jnp.dot(row_block, up_weight, preferred_element_type=jnp.float32)
        hidden = (jax.nn.silu(gate_vals) * up_vals).astype(jnp.bfloat16)
        return jnp.dot(hidden, down_weight, preferred_element_type=jnp.float32).astype(jnp.bfloat16)
    results = lax.map(one_expert, (slot_table.reshape(EXPERTS, block_count * CAP), routed_gate_weight, routed_up_weight, routed_down_weight))
    results = results.reshape(EXPERTS * block_count * CAP, D)
    slot_pairs = slot_flat.reshape(token_count, TOPK)
    routed = jnp.zeros((token_count, D), jnp.float32)
    for copy_index in range(TOPK):
        routed = routed + routed_copy_weight[:, copy_index:copy_index + 1] * results[slot_pairs[:, copy_index]].astype(jnp.float32)
    shared_hidden = (jax.nn.silu(jnp.dot(normed, shared_gate_weight, preferred_element_type=jnp.float32)) * jnp.dot(normed, shared_up_weight, preferred_element_type=jnp.float32)).astype(jnp.bfloat16)
    shared = jnp.dot(shared_hidden, shared_down_weight, preferred_element_type=jnp.float32)
    return (routed + shared).astype(jnp.bfloat16)

def reference(queries, head_key_rows, head_value_rows, log_input_gate, forget_logits, head_forget_bias, extra_log_forget, output_gate_logits, head_norm_gain, mixer_output_weight, second_batch_input, expert_norm_gain, routed_expert_index, routed_copy_weight, routed_gate_weight, routed_up_weight, routed_down_weight, shared_gate_weight, shared_up_weight, shared_down_weight):
    mixer_first_output = mixer_portion(queries, head_key_rows, head_value_rows, log_input_gate, forget_logits, head_forget_bias, extra_log_forget, output_gate_logits, head_norm_gain, mixer_output_weight)
    moe_out = expert_part(second_batch_input, expert_norm_gain, routed_expert_index, routed_copy_weight, routed_gate_weight, routed_up_weight, routed_down_weight, shared_gate_weight, shared_up_weight, shared_down_weight)
    return (mixer_first_output, moe_out)
```

```python
import jax
import jax.numpy as jnp
from jax import lax
from jax.experimental import pallas as pl
from jax.experimental.pallas import tpu as pltpu
from jax.sharding import Mesh
from jax.sharding import PartitionSpec as P

EP = ("ep_0", "ep_1")
EP_TP = ("ep_0", "ep_1", "tp")
BLK = 128
F32 = jnp.float32
BF16 = jnp.bfloat16
NEG = -1e30


def split_two(x):
    hi = x.astype(BF16)
    return hi, (x - hi.astype(F32)).astype(BF16)


def dot(a, b, dims=(((1,), (0,)), ((), ()))):
    return lax.dot_general(a, b, dims, preferred_element_type=F32)


def exact_dot(a, b, dims=(((1,), (0,)), ((), ()))):
    return lax.dot_general(
        a, b, dims, precision=lax.Precision.HIGHEST, preferred_element_type=F32
    )


def iota(shape, dim):
    return lax.broadcasted_iota(jnp.int32, shape, dim)


def whole(shape):
    return pl.BlockSpec(shape, lambda *_: (0,) * len(shape))


def cost(flops, nbytes):
    return pl.CostEstimate(flops=int(flops), bytes_accessed=int(nbytes), transcendentals=0)


def slot_rows(idx, cap, experts):
    tokens = idx.shape[1]
    sub = iota((experts, tokens), 0)
    first = sub == idx[0:1, :]
    second = sub == idx[1:2, :]
    named = jnp.where(first | second, 1.0, 0.0).astype(BF16)
    before = jnp.where(iota((tokens, tokens), 0) < iota((tokens, tokens), 1), 1.0, 0.0)
    prior = dot(named, before.astype(BF16))
    places = [jnp.sum(jnp.where(hot, prior, 0.0), axis=0, keepdims=True) for hot in (first, second)]
    return [
        idx[j : j + 1, :] * (2 * cap) + places[j].astype(jnp.int32) for j in range(2)
    ]


def dispatch_body(cap, experts, x_ref, gain_ref, idx_ref, send_ref, normed_ref, rows_ref, both_ref, want_ref):
    step = pl.program_id(0)
    tokens, width = x_ref.shape
    half = width // 2

    @pl.when(step == 0)
    def _():
        x = x_ref[...].astype(F32)
        scale = lax.rsqrt(jnp.mean(x * x, axis=-1, keepdims=True) + 1e-06)
        normed = (x * scale * gain_ref[...]).astype(BF16)
        normed_ref[...] = normed
        both_ref[0:tokens, :] = normed[:, :half]
        both_ref[tokens:, :] = normed[:, half:]
        row0, row1 = slot_rows(idx_ref[...], cap, experts)
        rows_ref[...] = jnp.concatenate([row0, row1, row0, row1, row0, row1, row0, row1], axis=0)
        want_ref[0:1, 0:tokens] = row0
        want_ref[1:2, 0:tokens] = row1

    rows = send_ref.shape[0]
    row = iota((rows, tokens), 0) + step * rows
    t0, t1 = want_ref[0:1, 0:tokens], want_ref[1:2, 0:tokens]
    low = jnp.where((row == t0) | (row == t1), 1.0, 0.0).astype(BF16)
    high = jnp.where((row == t0 + cap) | (row == t1 + cap), 1.0, 0.0).astype(BF16)
    out = dot(low, both_ref[0:tokens, :]) + dot(high, both_ref[tokens:, :])
    send_ref[...] = out.astype(BF16)


def dispatch_rows(x, gain, idx, cap, experts):
    tokens, width = x.shape
    total = experts * cap * 2
    steps = 4
    body = lambda *refs: dispatch_body(cap, experts, *refs)
    return pl.pallas_call(
        body,
        grid=(steps,),
        in_specs=[whole((tokens, width)), whole((1, width)), whole((2, tokens))],
        out_specs=[
            pl.BlockSpec((total // steps, width // 2), lambda i: (i, 0)),
            whole((tokens, width)),
            whole((8, tokens)),
        ],
        out_shape=[
            jax.ShapeDtypeStruct((total, width // 2), BF16),
            jax.ShapeDtypeStruct((tokens, width), BF16),
            jax.ShapeDtypeStruct((8, tokens), jnp.int32),
        ],
        scratch_shapes=[pltpu.VMEM((2 * tokens, width // 2), BF16), pltpu.VMEM((8, 256), jnp.int32)],
        compiler_params=pltpu.CompilerParams(dimension_semantics=("arbitrary",)),
        cost_estimate=cost(2 * total * tokens * width, 4 * total * width),
        name="dispatch_rows",
    )(x, gain, idx)


def swap_halves(even, odd, lower):
    first = jnp.where(lower, even, pltpu.roll(odd, 4, 1))
    last = jnp.where(lower, pltpu.roll(even, 4, 1), odd)
    return first, last


def expert_body(a_ref, g_ref, u_ref, d_ref, out_ref, x_ref, acc_ref):
    step = pl.program_id(0)
    pairs = a_ref.shape[0]
    half = a_ref.shape[3]
    group = 8
    lower = iota((group, 8, half), 1) < 4

    @pl.when(step == 0)
    def _():
        for i in range(pairs // group):
            tiles = a_ref[i * group : (i + 1) * group].astype(F32)
            first, last = swap_halves(tiles[:, 0], tiles[:, 1], lower)
            at = slice(i * group * 8, (i + 1) * group * 8)
            x_ref[at, 0:half] = first.reshape(group * 8, half).astype(BF16)
            x_ref[at, half:] = last.reshape(group * 8, half).astype(BF16)

    x = x_ref[...]
    gate = dot(x, g_ref[0])
    up = dot(x, u_ref[0])
    hidden = (gate * jax.nn.sigmoid(gate) * up).astype(BF16)
    part = dot(hidden, d_ref[0])

    @pl.when(step == 0)
    def _():
        acc_ref[...] = part

    @pl.when(step > 0)
    def _():
        acc_ref[...] += part

    @pl.when(step == pl.num_programs(0) - 1)
    def _():
        for i in range(pairs // group):
            at = slice(i * group * 8, (i + 1) * group * 8)
            first = acc_ref[at, 0:half].reshape(group, 8, half)
            last = acc_ref[at, half:].reshape(group, 8, half)
            even, odd = swap_halves(first, last, lower)
            out_ref[i * group : (i + 1) * group, 0] = even.astype(BF16)
            out_ref[i * group : (i + 1) * group, 1] = odd.astype(BF16)


def expert_products(arrived, gate_weight, up_weight, down_weight):
    count, rows, half = arrived.shape
    _, width, hidden = gate_weight.shape
    steps = 4
    piece = hidden // steps
    shape = (count // 2, 2, rows, half)
    out = pl.pallas_call(
        expert_body,
        grid=(steps,),
        in_specs=[
            whole(shape),
            pl.BlockSpec((1, width, piece), lambda i: (0, 0, i)),
            pl.BlockSpec((1, width, piece), lambda i: (0, 0, i)),
            pl.BlockSpec((1, piece, width), lambda i: (0, i, 0)),
        ],
        out_specs=whole(shape),
        out_shape=jax.ShapeDtypeStruct(shape, BF16),
        scratch_shapes=[
            pltpu.VMEM((count * rows // 2, width), BF16),
            pltpu.VMEM((count * rows // 2, width), F32),
        ],
        compiler_params=pltpu.CompilerParams(dimension_semantics=("arbitrary",)),
        cost_estimate=cost(3 * count * rows * width * hidden, 6 * width * hidden),
        name="expert_products",
    )(arrived.reshape(shape), gate_weight, up_weight, down_weight)
    return out.reshape(arrived.shape)


def shared_body(n_ref, g_ref, u_ref, d_ref, out_ref):
    normed = n_ref[...]
    gate = dot(normed, g_ref[...])
    up = dot(normed, u_ref[...])
    hidden = (gate * jax.nn.sigmoid(gate) * up).astype(BF16)
    out_ref[...] = dot(hidden, d_ref[...])


def shared_expert(normed, gate_weight, up_weight, down_weight):
    tokens, width = normed.shape
    hidden = gate_weight.shape[1]
    return pl.pallas_call(
        shared_body,
        out_shape=jax.ShapeDtypeStruct((tokens, width), F32),
        cost_estimate=cost(6 * tokens * width * hidden, 6 * width * hidden),
        name="shared_expert",
    )(normed, gate_weight, up_weight, down_weight)


def combine_body(cap, back_ref, rows_ref, weight_ref, shared_ref, out_ref):
    tokens, width = out_ref.shape
    half = width // 2
    total = back_ref.shape[0]
    row_col = jnp.transpose(jnp.concatenate([rows_ref[...].astype(F32)], axis=0))
    weights = jnp.concatenate([weight_ref[...]] * 4, axis=0)
    weight_col = jnp.transpose(weights)
    at0, at1 = row_col[:, 0:1].astype(jnp.int32), row_col[:, 1:2].astype(jnp.int32)
    w0, w1 = weight_col[:, 0:1], weight_col[:, 1:2]
    lane = iota((tokens, total), 1)
    parts = []
    for h in range(2):
        mixed = jnp.where(lane == at0 + h * cap, w0, 0.0) + jnp.where(lane == at1 + h * cap, w1, 0.0)
        parts.extend(split_two(mixed))
    product = dot(jnp.concatenate(parts, axis=0), back_ref[...])
    for h in range(2):
        routed = product[2 * h * tokens : (2 * h + 1) * tokens] + product[
            (2 * h + 1) * tokens : (2 * h + 2) * tokens
        ]
        cols = slice(h * half, (h + 1) * half)
        out_ref[:, cols] = (routed + shared_ref[:, cols]).astype(BF16)


def combine(back, rows, weights, shared, cap):
    tokens, width = shared.shape
    body = lambda *refs: combine_body(cap, *refs)
    return pl.pallas_call(
        body,
        out_shape=jax.ShapeDtypeStruct((tokens, width), BF16),
        cost_estimate=cost(8 * tokens * back.shape[0] * width // 2, 2 * back.size),
        name="combine",
    )(back, rows, weights, shared)


def gate_rows(in_ref, forget_ref, extra_ref, bias_ref):
    x = forget_ref[...] + bias_ref[0]
    log_forget = jnp.minimum(x, 0.0) - jnp.log1p(jnp.exp(-jnp.abs(x))) + extra_ref[...]
    upper = jnp.where(iota((BLK, BLK), 0) <= iota((BLK, BLK), 1), 1.0, 0.0)
    cumulative = exact_dot(log_forget, upper)
    ones = jnp.ones((BLK, BLK), F32)
    total = exact_dot(log_forget, ones)
    return in_ref[...], cumulative, total


def state_body(k_ref, v_ref, in_ref, forget_ref, extra_ref, bias_ref, out_ref):
    key_dim, length = k_ref.shape
    blocks = length // BLK
    in_gate, cumulative, total = gate_rows(in_ref, forget_ref, extra_ref, bias_ref)
    sums = [jnp.zeros((1, BLK), F32)]
    for j in reversed(range(1, blocks)):
        sums.insert(0, sums[0] + total[j : j + 1, :])
    after = jnp.concatenate(sums, axis=0)
    gap = after + total - cumulative + in_gate
    top = jnp.max(jnp.max(gap, axis=1, keepdims=True), axis=0, keepdims=True)
    weight = jnp.exp(gap - top)
    decay = jnp.sum(total[:, 0:1], axis=0, keepdims=True)
    acc = jnp.zeros((2 * key_dim, 2 * BLK), F32)
    ones = jnp.ones((2 * BLK, BLK), BF16)
    for j in range(blocks // 2):
        at = slice(j * 2 * BLK, (j + 1) * 2 * BLK)
        weights = jnp.concatenate([weight[2 * j : 2 * j + 1], weight[2 * j + 1 : 2 * j + 2]], axis=1)
        keys = k_ref[:, at].astype(F32) * weights
        hi, lo = split_two(keys)
        values = jnp.concatenate([v_ref[at, :], ones], axis=1)
        acc = acc + dot(jnp.concatenate([hi, lo], axis=0), values)
    state = acc[:key_dim] + acc[key_dim:]
    norm = jnp.transpose(state[:, BLK:])[0:8, :]
    norm = jnp.concatenate([norm, jnp.zeros((8, BLK - key_dim), F32)], axis=1)
    lane = iota((8, BLK), 1)
    tail = jnp.where(lane < key_dim, norm, jnp.where(lane < key_dim + 32, top, decay))
    for p in range(out_ref.shape[0]):
        out_ref[p, 0:key_dim, :] = state[:, 0:BLK]
        out_ref[p, key_dim:, :] = tail


def device_state(keys, values, in_gate, forget, extra, bias, copies):
    key_dim, length = keys.shape
    return pl.pallas_call(
        state_body,
        in_specs=[pl.BlockSpec(memory_space=pltpu.VMEM)] * 5 + [pl.BlockSpec(memory_space=pltpu.SMEM)],
        out_shape=jax.ShapeDtypeStruct((copies, key_dim + 8, BLK), F32),
        cost_estimate=cost(8 * length * key_dim * BLK, 4 * length * BLK),
        name="device_state",
    )(keys, values, in_gate, forget, extra, bias)


def incoming_state(states_ref, place, key_dim):
    count = states_ref.shape[0]
    tails = [states_ref[p, key_dim : key_dim + 1, :] for p in range(count)]
    tops = [t[:, key_dim : key_dim + 1] for t in tails]
    decays = [t[:, key_dim + 32 : key_dim + 33] for t in tails]
    since = jnp.zeros((1, 1), F32)
    gaps = [None] * count
    for p in reversed(range(count)):
        counted = jnp.full((1, 1), p, jnp.int32) < place
        gaps[p] = jnp.where(counted, tops[p] + since, NEG)
        since = since + jnp.where(counted, decays[p], 0.0)
    top = gaps[0]
    for p in range(1, count):
        top = jnp.maximum(top, gaps[p])
    memory = jnp.zeros((key_dim + 8, BLK), F32)
    for p in range(count):
        counted = jnp.full((1, 1), p, jnp.int32) < place
        scale = jnp.where(counted, jnp.exp(gaps[p] - top), 0.0)
        memory = memory + states_ref[p] * scale
    norm = jnp.broadcast_to(memory[key_dim : key_dim + 1, :], (BLK, BLK))
    norm = jnp.transpose(norm)[0:key_dim, :]
    return jnp.concatenate([memory[0:key_dim], norm], axis=1), top


def mixer_body(
    place_ref,
    bias_ref,
    states_ref,
    q_ref,
    k_ref,
    v_ref,
    in_ref,
    forget_ref,
    extra_ref,
    gate_ref,
    gain_ref,
    out_ref,
):
    key_dim, length = k_ref.shape
    blocks = length // BLK
    tokens = length // out_ref.shape[0]
    per_chunk = tokens // BLK
    in_gate, cumulative, total = gate_rows(in_ref, forget_ref, extra_ref, bias_ref)
    state, top = incoming_state(states_ref, place_ref[0], key_dim)
    gap = total - cumulative + in_gate
    block_top = jnp.max(gap, axis=1, keepdims=True)
    weight = jnp.exp(gap - block_top)
    shifted = in_gate - cumulative
    sum_col = jnp.transpose(jnp.concatenate([cumulative] * (BLK // blocks), axis=0))
    ones = jnp.ones((BLK, BLK), BF16)
    lower = iota((BLK, BLK), 1) <= iota((BLK, BLK), 0)
    gain = gain_ref[...]
    eight = jnp.ones((8, BLK), F32)
    squares = []
    for j in range(blocks):
        at = slice(j * BLK, (j + 1) * BLK)
        keys = k_ref[:, at]
        values = jnp.concatenate([v_ref[at, :], ones], axis=1)
        query = jnp.transpose(q_ref[:, at].astype(F32) * (key_dim**-0.5)).astype(BF16)
        base = sum_col[:, j : j + 1]
        pair = jnp.where(lower, base + shifted[j : j + 1, :], -jnp.inf)
        carried = base + top
        stable = jnp.maximum(carried, jnp.max(pair, axis=1, keepdims=True))
        scores = dot(query, keys) * jnp.exp(pair - stable)
        carry = jnp.exp(carried - stable)
        score_hi, score_lo = split_two(scores)
        state_hi, state_lo = split_two(state)
        both = dot(score_hi, values) + dot(score_lo, values)
        both = both + carry * (dot(query, state_hi) + dot(query, state_lo))
        hidden = both[:, :BLK] / jnp.maximum(jnp.abs(both[:, BLK:]), jnp.exp(-stable))
        squares.append(
            exact_dot(eight, hidden * hidden, (((1,), (1,)), ((), ())))[0:1, :]
        )
        gated = hidden * gain * jax.nn.sigmoid(gate_ref[at, :].astype(F32))
        start = (j % per_chunk) * BLK
        out_ref[j // per_chunk, start : start + BLK, :] = gated.astype(BF16)
        if j + 1 < blocks:
            hi, lo = split_two(keys.astype(F32) * weight[j : j + 1, :])
            added = dot(jnp.concatenate([hi, lo], axis=0), values)
            added = added[:key_dim] + added[key_dim:]
            late = block_top[j : j + 1, :]
            early = total[j : j + 1, 0:1] + top
            top = jnp.maximum(early, late)
            state = jnp.exp(early - top) * state + jnp.exp(late - top) * added
    for c in range(out_ref.shape[0]):
        own = squares[c * per_chunk : (c + 1) * per_chunk]
        parts = [split_two(row) for row in own]
        rows = [hi.astype(F32) for hi, _ in parts] + [lo.astype(F32) for _, lo in parts]
        rows.append(jnp.zeros((16 - len(rows), BLK), F32))
        out_ref[c, tokens:, :] = jnp.concatenate(rows, axis=0).astype(BF16)


def mixer_rows(place, bias, states, queries, keys, values, in_gate, forget, extra, gate, gain, peers):
    key_dim, length = keys.shape
    smem = pl.BlockSpec(memory_space=pltpu.SMEM)
    vmem = pl.BlockSpec(memory_space=pltpu.VMEM)
    return pl.pallas_call(
        mixer_body,
        in_specs=[smem, smem] + [vmem] * 9,
        out_shape=jax.ShapeDtypeStruct((peers, length // peers + 16, BLK), BF16),
        cost_estimate=cost(32 * length * BLK * BLK, 8 * length * BLK),
        name="mixer_rows",
    )(place, bias, states, queries, keys, values, in_gate, forget, extra, gate, gain)


def project_body(g_ref, w_ref, out_ref):
    heads = g_ref.shape[0]
    tokens = out_ref.shape[0]
    per_chunk = tokens // BLK
    tail = g_ref[0, tokens:, :].astype(F32)
    for h in range(1, heads):
        tail = tail + g_ref[h, tokens:, :].astype(F32)
    columns = []
    for c in range(per_chunk):
        row = tail[c : c + 1, :] + tail[per_chunk + c : per_chunk + c + 1, :]
        row = lax.rsqrt(row / (heads * BLK) + 1e-06)
        columns.append(jnp.transpose(jnp.broadcast_to(row, (BLK, BLK)))[:, 0:1])
    scale = jnp.concatenate(columns, axis=0)
    mixed = jnp.concatenate([g_ref[h, 0:tokens, :] for h in range(heads)], axis=1)
    out_ref[...] = (dot(mixed, w_ref[...]) * scale).astype(BF16)


def project(gathered, weight):
    heads, rows, _ = gathered.shape
    width = weight.shape[1]
    steps = 4
    return pl.pallas_call(
        project_body,
        grid=(steps,),
        in_specs=[
            whole(gathered.shape),
            pl.BlockSpec((weight.shape[0], width // steps), lambda i: (0, i)),
        ],
        out_specs=pl.BlockSpec((rows - 16, width // steps), lambda i: (0, i)),
        out_shape=jax.ShapeDtypeStruct((rows - 16, width), BF16),
        compiler_params=pltpu.CompilerParams(dimension_semantics=("arbitrary",)),
        cost_estimate=cost(2 * (rows - 16) * weight.size, 2 * weight.size),
        name="project",
    )(gathered, weight)


def exchange(x, axes):
    return lax.all_to_all(x, axes, split_axis=0, concat_axis=0, tiled=True)


def on_device(
    queries,
    head_key_rows,
    head_value_rows,
    log_input_gate,
    forget_logits,
    head_forget_bias,
    extra_log_forget,
    output_gate_logits,
    head_norm_gain,
    mixer_output_weight,
    second_batch_input,
    expert_norm_gain,
    routed_expert_index,
    routed_copy_weight,
    routed_gate_weight,
    routed_up_weight,
    routed_down_weight,
    shared_gate_weight,
    shared_up_weight,
    shared_down_weight,
):
    length = queries.shape[0]
    ep_count, tp_count = lax.axis_size(EP), lax.axis_size("tp")
    experts = ep_count * tp_count
    cap = 4
    send, normed, rows = dispatch_rows(
        second_batch_input, expert_norm_gain[None, :], routed_expert_index.T, cap, experts
    )
    landed = exchange(send.reshape(experts, 2 * cap, -1), EP_TP)

    def by_block(a):
        return a.reshape(length // BLK, BLK)

    in_gate, forget, extra = (
        by_block(log_input_gate),
        by_block(forget_logits),
        by_block(extra_log_forget),
    )
    query_rows, key_rows = queries.T, head_key_rows.T
    copies = device_state(
        key_rows, head_value_rows, in_gate, forget, extra, head_forget_bias, ep_count
    )
    states = exchange(copies, EP)
    shared = shared_expert(normed, shared_gate_weight, shared_up_weight, shared_down_weight)
    place = lax.axis_index(EP).astype(jnp.int32).reshape(1)
    mixed = mixer_rows(
        place,
        head_forget_bias,
        states,
        query_rows,
        key_rows,
        head_value_rows,
        in_gate,
        forget,
        extra,
        output_gate_logits,
        head_norm_gain[None, :],
        tp_count,
    )
    gathered = exchange(mixed, "tp")
    produced = expert_products(landed, routed_gate_weight, routed_up_weight, routed_down_weight)
    back = exchange(produced, EP_TP)
    mixer_first_output = project(gathered, mixer_output_weight)
    moe_out = combine(
        back.reshape(experts * 2 * cap, -1), rows, routed_copy_weight.T, shared, cap
    )
    return (mixer_first_output, moe_out)


def solution(mesh):
    split = Mesh(mesh.devices.reshape(4, 4, mesh.shape["tp"]), ("ep_0", "ep_1", "tp"))
    return jax.shard_map(
        on_device,
        mesh=split,
        in_specs=(
            P(EP, "tp"),
            P(EP, "tp"),
            P(EP, "tp"),
            P(EP, "tp"),
            P(EP, "tp"),
            P("tp"),
            P(EP, "tp"),
            P(EP, "tp"),
            P("tp"),
            P(),
            P(EP_TP, None),
            P(),
            P(EP_TP, None),
            P(EP_TP, None),
            P(EP_TP, None, None),
            P(EP_TP, None, None),
            P(EP_TP, None, None),
            P(),
            P(),
            P(),
        ),
        out_specs=(P(EP_TP, None), P(EP_TP, None)),
        check_vma=False,
    )
```

```python
import jax
import jax.numpy as jnp
from jax import lax
from jax.experimental import pallas as pl
from jax.experimental.pallas import tpu as pltpu
from jax.sharding import Mesh
from jax.sharding import PartitionSpec as P


EP = ("ep_0", "ep_1")
EP_TP = ("ep_0", "ep_1", "tp")
BLK = 128
F32 = jnp.float32
BF16 = jnp.bfloat16
NEG = -1e30


def split_two(x):
    hi = x.astype(BF16)
    return hi, (x - hi.astype(F32)).astype(BF16)


def dot(a, b, dims=(((1,), (0,)), ((), ()))):
    return lax.dot_general(a, b, dims, preferred_element_type=F32)


def exact_dot(a, b, dims=(((1,), (0,)), ((), ()))):
    return lax.dot_general(
        a, b, dims, precision=lax.Precision.HIGHEST, preferred_element_type=F32
    )


def iota(shape, dim):
    return lax.broadcasted_iota(jnp.int32, shape, dim)


def whole(shape):
    return pl.BlockSpec(shape, lambda *_: (0,) * len(shape))


def params(mib, grid=False):
    return pltpu.CompilerParams(
        vmem_limit_bytes=mib * 2**20,
        dimension_semantics=("arbitrary",) if grid else None,
    )


def in_hbm(*arrays):
    return [pltpu.with_memory_space_constraint(a, pltpu.HBM) for a in arrays]


def cost(flops, nbytes):
    return pl.CostEstimate(flops=int(flops), bytes_accessed=int(nbytes), transcendentals=0)


def slot_rows(idx, cap, experts):
    tokens = idx.shape[1]
    sub = iota((experts, tokens), 0)
    first = sub == idx[0:1, :]
    second = sub == idx[1:2, :]
    named = jnp.where(first | second, 1.0, 0.0).astype(BF16)
    before = jnp.where(iota((tokens, tokens), 0) < iota((tokens, tokens), 1), 1.0, 0.0)
    prior = dot(named, before.astype(BF16))
    places = [jnp.sum(jnp.where(hot, prior, 0.0), axis=0, keepdims=True) for hot in (first, second)]
    return [
        idx[j : j + 1, :] * (2 * cap) + places[j].astype(jnp.int32) for j in range(2)
    ]


def dispatch_body(cap, experts, x_ref, gain_ref, idx_ref, send_ref, normed_ref, rows_ref, both_ref, want_ref):
    step = pl.program_id(0)
    tokens, width = x_ref.shape
    half = width // 2

    @pl.when(step == 0)
    def _():
        x = x_ref[...].astype(F32)
        scale = lax.rsqrt(jnp.mean(x * x, axis=-1, keepdims=True) + 1e-06)
        normed = (x * scale * gain_ref[...]).astype(BF16)
        normed_ref[...] = normed
        both_ref[0:tokens, :] = normed[:, :half]
        both_ref[tokens:, :] = normed[:, half:]
        row0, row1 = slot_rows(idx_ref[...], cap, experts)
        rows_ref[...] = jnp.concatenate([row0, row1, row0, row1, row0, row1, row0, row1], axis=0)
        want_ref[0:1, 0:tokens] = row0
        want_ref[1:2, 0:tokens] = row1

    rows = send_ref.shape[0]
    row = iota((rows, tokens), 0) + step * rows
    t0, t1 = want_ref[0:1, 0:tokens], want_ref[1:2, 0:tokens]
    low = jnp.where((row == t0) | (row == t1), 1.0, 0.0).astype(BF16)
    high = jnp.where((row == t0 + cap) | (row == t1 + cap), 1.0, 0.0).astype(BF16)
    out = dot(low, both_ref[0:tokens, :]) + dot(high, both_ref[tokens:, :])
    send_ref[...] = out.astype(BF16)


def dispatch_rows(x, gain, idx, cap, experts):
    tokens, width = x.shape
    total = experts * cap * 2
    steps = 4
    body = lambda *refs: dispatch_body(cap, experts, *refs)
    return pl.pallas_call(
        body,
        grid=(steps,),
        in_specs=[whole((tokens, width)), whole((1, width)), whole((2, tokens))],
        out_specs=[
            pl.BlockSpec((total // steps, width // 2), lambda i: (i, 0)),
            whole((tokens, width)),
            whole((8, tokens)),
        ],
        out_shape=[
            pltpu.HBM((total, width // 2), BF16),
            pltpu.HBM((tokens, width), BF16),
            pltpu.HBM((8, tokens), jnp.int32),
        ],
        scratch_shapes=[pltpu.VMEM((2 * tokens, width // 2), BF16), pltpu.VMEM((8, 256), jnp.int32)],
        compiler_params=params(20, True),
        cost_estimate=cost(2 * total * tokens * width, 4 * total * width),
        name="dispatch_rows",
    )(*in_hbm(x, gain, idx))


def swap_halves(even, odd, lower):
    first = jnp.where(lower, even, pltpu.roll(odd, 4, 1))
    last = jnp.where(lower, pltpu.roll(even, 4, 1), odd)
    return first, last


def expert_body(pieces, a_ref, g_hbm, u_hbm, d_hbm, out_hbm, x_ref, h_ref, g_ref, u_ref, d_ref, o_ref, sems):
    pairs = a_ref.shape[0]
    half = a_ref.shape[3]
    hidden = h_ref.shape[1]
    group = 8
    wide = hidden // pieces
    part = half // pieces
    first_loads, last_loads, stores = [], [], []
    for p in range(pieces):
        at = slice(p * wide, (p + 1) * wide)
        first_loads.append(
            [
                pltpu.make_async_copy(g_hbm.at[0, :, at], g_ref.at[p], sems.at[0, p]),
                pltpu.make_async_copy(u_hbm.at[0, :, at], u_ref.at[p], sems.at[1, p]),
            ]
        )
        at = slice(p * part, (p + 1) * part)
        other = slice(half + p * part, half + (p + 1) * part)
        last_loads.append(
            [
                pltpu.make_async_copy(d_hbm.at[0, :, at], d_ref.at[p, 0], sems.at[2, p]),
                pltpu.make_async_copy(d_hbm.at[0, :, other], d_ref.at[p, 1], sems.at[3, p]),
            ]
        )
        stores.append(pltpu.make_async_copy(o_ref.at[p], out_hbm.at[:, :, :, at], sems.at[4, p]))
    loads = first_loads + last_loads
    ahead = 3
    for copies in loads[:ahead]:
        for copy in copies:
            copy.start()
    lower = iota((group, 8, half), 1) < 4
    for i in range(pairs // group):
        tiles = a_ref[i * group : (i + 1) * group].astype(F32)
        first, last = swap_halves(tiles[:, 0], tiles[:, 1], lower)
        at = slice(i * group * 8, (i + 1) * group * 8)
        x_ref[at, 0:half] = first.reshape(group * 8, half).astype(BF16)
        x_ref[at, half:] = last.reshape(group * 8, half).astype(BF16)

    def arrive(n):
        for copy in loads[n]:
            copy.wait()
        if n + ahead < len(loads):
            for copy in loads[n + ahead]:
                copy.start()

    for p in range(pieces):
        arrive(p)
        x = x_ref[...]
        gate = dot(x, g_ref[p])
        up = dot(x, u_ref[p])
        h_ref[:, p * wide : (p + 1) * wide] = (gate * jax.nn.sigmoid(gate) * up).astype(BF16)
    lower = iota((pairs, 8, part), 1) < 4
    for p in range(pieces):
        arrive(pieces + p)
        h = h_ref[...]
        first = dot(h, d_ref[p, 0]).reshape(pairs, 8, part)
        last = dot(h, d_ref[p, 1]).reshape(pairs, 8, part)
        even, odd = swap_halves(first, last, lower)
        o_ref[p, :, 0] = even.astype(BF16)
        o_ref[p, :, 1] = odd.astype(BF16)
        stores[p].start()
    for store in stores:
        store.wait()


def expert_products(arrived, gate_weight, up_weight, down_weight):
    count, rows, half = arrived.shape
    _, width, hidden = gate_weight.shape
    pieces = 4
    shape = (count // 2, 2, rows, half)
    slots = count * rows // 2
    hbm = pl.BlockSpec(memory_space=pltpu.HBM)
    body = lambda *refs: expert_body(pieces, *refs)
    out = pl.pallas_call(
        body,
        in_specs=[pl.BlockSpec(memory_space=pltpu.VMEM), hbm, hbm, hbm],
        out_specs=hbm,
        out_shape=pltpu.HBM(shape, BF16),
        scratch_shapes=[
            pltpu.VMEM((slots, width), BF16),
            pltpu.VMEM((slots, hidden), BF16),
            pltpu.VMEM((pieces, width, hidden // pieces), BF16),
            pltpu.VMEM((pieces, width, hidden // pieces), BF16),
            pltpu.VMEM((pieces, 2, hidden, half // pieces), BF16),
            pltpu.VMEM((pieces, count // 2, 2, rows, half // pieces), BF16),
            pltpu.SemaphoreType.DMA((5, pieces)),
        ],
        compiler_params=params(32),
        cost_estimate=cost(3 * count * rows * width * hidden, 6 * width * hidden),
        name="expert_products",
    )(arrived.reshape(shape), *in_hbm(gate_weight, up_weight, down_weight))
    return out.reshape(arrived.shape)


def shared_body(n_ref, g_ref, u_ref, d_ref, out_ref):
    normed = n_ref[...]
    gate = dot(normed, g_ref[...])
    up = dot(normed, u_ref[...])
    hidden = (gate * jax.nn.sigmoid(gate) * up).astype(BF16)
    out_ref[...] = dot(hidden, d_ref[...])


def shared_expert(normed, gate_weight, up_weight, down_weight):
    tokens, width = normed.shape
    hidden = gate_weight.shape[1]
    return pl.pallas_call(
        shared_body,
        out_shape=pltpu.HBM((tokens, width), F32),
        compiler_params=params(16),
        cost_estimate=cost(6 * tokens * width * hidden, 6 * width * hidden),
        name="shared_expert",
    )(*in_hbm(normed, gate_weight, up_weight, down_weight))


def combine_body(cap, back_ref, rows_ref, weight_ref, shared_hbm, out_hbm, shared_ref, out_ref, sems):
    tokens, _ = out_ref.shape
    total, half = back_ref.shape
    loads, stores = [], []
    for h in range(2):
        cols = slice(h * half, (h + 1) * half)
        loads.append(
            pltpu.make_async_copy(shared_hbm.at[:, cols], shared_ref.at[:, cols], sems.at[0, h])
        )
        stores.append(pltpu.make_async_copy(out_ref.at[:, cols], out_hbm.at[:, cols], sems.at[1, h]))
        loads[h].start()
    row_col = jnp.transpose(rows_ref[...].astype(F32))
    weight_col = jnp.transpose(jnp.concatenate([weight_ref[...]] * 4, axis=0))
    at0, at1 = row_col[:, 0:1].astype(jnp.int32), row_col[:, 1:2].astype(jnp.int32)
    w0, w1 = weight_col[:, 0:1], weight_col[:, 1:2]
    lane = iota((tokens, total), 1)
    for h in range(2):
        cols = slice(h * half, (h + 1) * half)
        mixed = jnp.where(lane == at0 + h * cap, w0, jnp.where(lane == at1 + h * cap, w1, 0.0))
        product = dot(jnp.concatenate(split_two(mixed), axis=0), back_ref[...])
        loads[h].wait()
        routed = product[0:tokens] + product[tokens:]
        out_ref[:, cols] = (routed + shared_ref[:, cols]).astype(BF16)
        stores[h].start()
    for store in stores:
        store.wait()


def combine(back, rows, weights, shared, cap):
    tokens, width = shared.shape
    hbm = pl.BlockSpec(memory_space=pltpu.HBM)
    vmem = pl.BlockSpec(memory_space=pltpu.VMEM)
    body = lambda *refs: combine_body(cap, *refs)
    return pl.pallas_call(
        body,
        in_specs=[vmem, vmem, vmem, hbm],
        out_specs=hbm,
        out_shape=jax.ShapeDtypeStruct((tokens, width), BF16),
        scratch_shapes=[
            pltpu.VMEM((tokens, width), F32),
            pltpu.VMEM((tokens, width), BF16),
            pltpu.SemaphoreType.DMA((2, 2)),
        ],
        compiler_params=params(20),
        cost_estimate=cost(4 * tokens * back.shape[0] * width, 2 * back.size),
        name="combine",
    )(back, rows, weights, *in_hbm(shared))


def gate_rows(in_ref, forget_ref, extra_ref, bias_ref):
    x = forget_ref[...] + bias_ref[0]
    log_forget = jnp.minimum(x, 0.0) - jnp.log1p(jnp.exp(-jnp.abs(x))) + extra_ref[...]
    upper = jnp.where(iota((BLK, BLK), 0) <= iota((BLK, BLK), 1), 1.0, 0.0)
    cumulative = exact_dot(log_forget, upper)
    ones = jnp.ones((BLK, BLK), F32)
    total = exact_dot(log_forget, ones)
    return in_ref[...], cumulative, total


def state_body(k_ref, v_ref, in_ref, forget_ref, extra_ref, bias_ref, out_ref):
    key_dim, length = k_ref.shape
    blocks = length // BLK
    in_gate, cumulative, total = gate_rows(in_ref, forget_ref, extra_ref, bias_ref)
    sums = [jnp.zeros((1, BLK), F32)]
    for j in reversed(range(1, blocks)):
        sums.insert(0, sums[0] + total[j : j + 1, :])
    after = jnp.concatenate(sums, axis=0)
    gap = after + total - cumulative + in_gate
    top = jnp.max(jnp.max(gap, axis=1, keepdims=True), axis=0, keepdims=True)
    weight = jnp.exp(gap - top)
    decay = jnp.sum(total[:, 0:1], axis=0, keepdims=True)
    acc = jnp.zeros((2 * key_dim, 2 * BLK), F32)
    ones = jnp.ones((2 * BLK, BLK), BF16)
    for j in range(blocks // 2):
        at = slice(j * 2 * BLK, (j + 1) * 2 * BLK)
        weights = jnp.concatenate([weight[2 * j : 2 * j + 1], weight[2 * j + 1 : 2 * j + 2]], axis=1)
        keys = k_ref[:, at].astype(F32) * weights
        hi, lo = split_two(keys)
        values = jnp.concatenate([v_ref[at, :], ones], axis=1)
        acc = acc + dot(jnp.concatenate([hi, lo], axis=0), values)
    state = acc[:key_dim] + acc[key_dim:]
    norm = jnp.transpose(state[:, BLK:])[0:8, :]
    norm = jnp.concatenate([norm, jnp.zeros((8, BLK - key_dim), F32)], axis=1)
    lane = iota((8, BLK), 1)
    tail = jnp.where(lane < key_dim, norm, jnp.where(lane < key_dim + 32, top, decay))
    out_ref[0:key_dim, :] = state[:, 0:BLK]
    out_ref[key_dim:, :] = tail


def device_state(keys, values, in_gate, forget, extra, bias):
    key_dim, length = keys.shape
    return pl.pallas_call(
        state_body,
        in_specs=[pl.BlockSpec(memory_space=pltpu.VMEM)] * 5 + [pl.BlockSpec(memory_space=pltpu.SMEM)],
        out_shape=jax.ShapeDtypeStruct((key_dim + 8, BLK), F32),
        compiler_params=params(8),
        cost_estimate=cost(8 * length * key_dim * BLK, 4 * length * BLK),
        name="device_state",
    )(*in_hbm(keys, values, in_gate, forget, extra), bias)


def merge_states(refs, keys, counted, key_dim):
    tails = [ref[key_dim : key_dim + 1, :] for ref in refs]
    tops = [t[:, key_dim : key_dim + 1] for t in tails]
    decays = [
        jnp.where(c, t[:, key_dim + 32 : key_dim + 33], 0.0) for t, c in zip(tails, counted)
    ]
    gaps = []
    for i, key in enumerate(keys):
        since = jnp.zeros((1, 1), F32)
        for j, other in enumerate(keys):
            if j != i:
                since = since + jnp.where(other > key, decays[j], 0.0)
        gaps.append(jnp.where(counted[i], tops[i] + since, NEG))
    top = gaps[0]
    for gap in gaps[1:]:
        top = jnp.maximum(top, gap)
    merged = jnp.zeros((key_dim + 8, BLK), F32)
    for ref, gap, c in zip(refs, gaps, counted):
        merged = merged + ref[...] * jnp.where(c, jnp.exp(gap - top), 0.0)
    return merged, top, sum(decays)


def as_one(scalar):
    return jnp.full((1, 1), scalar, jnp.int32)


def ring_places(place, count):
    return [as_one((place + count - k) % count) for k in range(count)]


def row_body(place_ref, *refs):
    *states, out_ref = refs
    key_dim = out_ref.shape[0] - 8
    keys = ring_places(place_ref[1], len(states))
    counted = [jnp.full((1, 1), True)] * len(states)
    merged, top, decay = merge_states(states, keys, counted, key_dim)
    lane = iota((8, BLK), 1)
    norm = merged[key_dim:, :]
    out_ref[0:key_dim, :] = merged[0:key_dim]
    out_ref[key_dim:, :] = jnp.where(
        lane < key_dim, norm, jnp.where(lane < key_dim + 32, top, decay)
    )


def row_state(place, states):
    return pl.pallas_call(
        row_body,
        in_specs=[pl.BlockSpec(memory_space=pltpu.SMEM)]
        + [pl.BlockSpec(memory_space=pltpu.VMEM)] * len(states),
        out_shape=jax.ShapeDtypeStruct(states[0].shape, F32),
        compiler_params=params(4),
        cost_estimate=cost(2**20, 2**18),
        name="row_state",
    )(place, *states)


def incoming_state(place_ref, rows, columns, key_dim):
    in_row = ring_places(place_ref[1], len(rows))
    in_column = ring_places(place_ref[0], len(columns) + 1)[1:]
    counted = [p < as_one(place_ref[1]) for p in in_row[1:]]
    counted += [p < as_one(place_ref[0]) for p in in_column]
    keys = [p + len(columns) + 1 for p in in_row[1:]] + in_column
    memory, top, _ = merge_states(rows[1:] + columns, keys, counted, key_dim)
    norm = jnp.broadcast_to(memory[key_dim : key_dim + 1, :], (BLK, BLK))
    norm = jnp.transpose(norm)[0:key_dim, :]
    return jnp.concatenate([memory[0:key_dim], norm], axis=1), top


def mixer_body(
    rows_count,
    columns_count,
    place_ref,
    bias_ref,
    q_ref,
    k_ref,
    v_ref,
    in_ref,
    forget_ref,
    extra_ref,
    gate_ref,
    gain_ref,
    *refs,
):
    key_dim, length = k_ref.shape
    blocks = length // BLK
    rows = list(refs[:rows_count])
    columns = list(refs[rows_count : rows_count + columns_count])
    out_ref = refs[-1]
    peers = out_ref.shape[0]
    tokens = length // peers
    per_chunk = tokens // BLK
    in_gate, cumulative, total = gate_rows(in_ref, forget_ref, extra_ref, bias_ref)
    state, top = incoming_state(place_ref, rows, columns, key_dim)
    gap = total - cumulative + in_gate
    block_top = jnp.max(gap, axis=1, keepdims=True)
    weight = jnp.exp(gap - block_top)
    shifted = in_gate - cumulative
    sum_col = jnp.transpose(jnp.concatenate([cumulative] * (BLK // blocks), axis=0))
    ones = jnp.ones((BLK, BLK), BF16)
    lower = iota((BLK, BLK), 1) <= iota((BLK, BLK), 0)
    gain = gain_ref[...]
    eight = jnp.ones((8, BLK), F32)
    squares = []
    for j in range(blocks):
        at = slice(j * BLK, (j + 1) * BLK)
        keys = k_ref[:, at]
        values = jnp.concatenate([v_ref[at, :], ones], axis=1)
        query = jnp.transpose(q_ref[:, at].astype(F32) * (key_dim**-0.5)).astype(BF16)
        base = sum_col[:, j : j + 1]
        pair = jnp.where(lower, base + shifted[j : j + 1, :], -jnp.inf)
        carried = base + top
        stable = jnp.maximum(carried, jnp.max(pair, axis=1, keepdims=True))
        scores = dot(query, keys) * jnp.exp(pair - stable)
        carry = jnp.exp(carried - stable)
        score_hi, score_lo = split_two(scores)
        state_hi, state_lo = split_two(state)
        both = dot(score_hi, values) + dot(score_lo, values)
        both = both + carry * (dot(query, state_hi) + dot(query, state_lo))
        hidden = both[:, :BLK] / jnp.maximum(jnp.abs(both[:, BLK:]), jnp.exp(-stable))
        squares.append(
            exact_dot(eight, hidden * hidden, (((1,), (1,)), ((), ())))[0:1, :]
        )
        gated = hidden * gain * jax.nn.sigmoid(gate_ref[at, :].astype(F32))
        start = (j % per_chunk) * BLK
        out_ref[j // per_chunk, start : start + BLK, :] = gated.astype(BF16)
        if j + 1 < blocks:
            hi, lo = split_two(keys.astype(F32) * weight[j : j + 1, :])
            added = dot(jnp.concatenate([hi, lo], axis=0), values)
            added = added[:key_dim] + added[key_dim:]
            late = block_top[j : j + 1, :]
            early = total[j : j + 1, 0:1] + top
            top = jnp.maximum(early, late)
            state = jnp.exp(early - top) * state + jnp.exp(late - top) * added
    for c in range(peers):
        own = squares[c * per_chunk : (c + 1) * per_chunk]
        parts = [split_two(row) for row in own]
        rows = [hi.astype(F32) for hi, _ in parts] + [lo.astype(F32) for _, lo in parts]
        rows.append(jnp.zeros((16 - len(rows), BLK), F32))
        out_ref[c, tokens:, :] = jnp.concatenate(rows, axis=0).astype(BF16)


def mixer_rows(place, bias, rows, columns, queries, keys, values, in_gate, forget, extra, gate, gain, peers):
    _, length = keys.shape
    smem = pl.BlockSpec(memory_space=pltpu.SMEM)
    vmem = pl.BlockSpec(memory_space=pltpu.VMEM)
    chunk = (length // peers + 16, BLK)
    body = lambda *refs: mixer_body(len(rows), len(columns), *refs)
    return pl.pallas_call(
        body,
        in_specs=[smem, smem] + [vmem] * (8 + len(rows) + len(columns)),
        out_shape=pltpu.HBM((peers, *chunk), BF16),
        compiler_params=params(16),
        cost_estimate=cost(32 * length * BLK * BLK, 8 * length * BLK),
        name="mixer_rows",
    )(
        place,
        bias,
        *in_hbm(queries, keys, values, in_gate, forget, extra, gate, gain),
        *rows,
        *columns,
    )


def project_body(g_ref, w_ref, out_ref, scale_ref):
    heads = g_ref.shape[0]
    tokens = out_ref.shape[0]
    per_chunk = tokens // BLK

    @pl.when(pl.program_id(0) == 0)
    def _():
        tail = g_ref[0, tokens:, :].astype(F32)
        for h in range(1, heads):
            tail = tail + g_ref[h, tokens:, :].astype(F32)
        for c in range(per_chunk):
            row = tail[c : c + 1, :] + tail[per_chunk + c : per_chunk + c + 1, :]
            row = lax.rsqrt(row / (heads * BLK) + 1e-06)
            scale_ref[c * BLK : (c + 1) * BLK, :] = jnp.transpose(jnp.broadcast_to(row, (BLK, BLK)))

    mixed = jnp.concatenate([g_ref[h, 0:tokens, :] for h in range(heads)], axis=1)
    product = dot(mixed, w_ref[...])
    out_ref[...] = (product * scale_ref[:, 0:1]).astype(BF16)


def project(gathered, weight):
    _, rows, _ = gathered.shape
    tokens = rows - 16
    width = weight.shape[1]
    steps = 4
    return pl.pallas_call(
        project_body,
        grid=(steps,),
        in_specs=[
            whole(gathered.shape),
            pl.BlockSpec((weight.shape[0], width // steps), lambda i: (0, i)),
        ],
        out_specs=pl.BlockSpec((tokens, width // steps), lambda i: (0, i)),
        out_shape=jax.ShapeDtypeStruct((tokens, width), BF16),
        scratch_shapes=[pltpu.VMEM((tokens, BLK), F32)],
        compiler_params=params(16, True),
        cost_estimate=cost(2 * tokens * weight.size, 2 * weight.size),
        name="project",
    )(gathered, *in_hbm(weight))


def exchange(x, axes):
    return lax.all_to_all(x, axes, split_axis=0, concat_axis=0, tiled=True)


def from_earlier(x, axis):
    count = lax.axis_size(axis)
    return [
        lax.ppermute(x, axis, [(p, (p + k) % count) for p in range(count)])
        for k in range(1, count)
    ]


def on_one(
    queries,
    head_key_rows,
    head_value_rows,
    log_input_gate,
    forget_logits,
    head_forget_bias,
    extra_log_forget,
    output_gate_logits,
    head_norm_gain,
    mixer_output_weight,
    second_batch_input,
    expert_norm_gain,
    routed_expert_index,
    routed_copy_weight,
    routed_gate_weight,
    routed_up_weight,
    routed_down_weight,
    shared_gate_weight,
    shared_up_weight,
    shared_down_weight,
):
    length = queries.shape[0]
    ep_count, tp_count = lax.axis_size(EP), lax.axis_size("tp")
    experts = ep_count * tp_count
    cap = 4
    send, normed, rows = dispatch_rows(
        second_batch_input, expert_norm_gain[None, :], routed_expert_index.T, cap, experts
    )
    landed = exchange(send.reshape(experts, 2 * cap, -1), EP_TP)

    def by_block(a):
        return a.reshape(length // BLK, BLK)

    in_gate, forget, extra = (
        by_block(log_input_gate),
        by_block(forget_logits),
        by_block(extra_log_forget),
    )
    query_rows, key_rows = queries.T, head_key_rows.T
    place = jnp.stack([lax.axis_index(a).astype(jnp.int32) for a in ("ep_0", "ep_1", "tp")])
    own = device_state(key_rows, head_value_rows, in_gate, forget, extra, head_forget_bias)
    row_states = [own] + from_earlier(own, "ep_1")
    row_total = row_state(place, row_states)
    column_states = from_earlier(row_total, "ep_0")
    mixed = mixer_rows(
        place,
        head_forget_bias,
        row_states,
        column_states,
        query_rows,
        key_rows,
        head_value_rows,
        in_gate,
        forget,
        extra,
        output_gate_logits,
        head_norm_gain[None, :],
        tp_count,
    )
    shared = shared_expert(normed, shared_gate_weight, shared_up_weight, shared_down_weight)
    gathered = exchange(mixed, "tp")
    produced = expert_products(landed, routed_gate_weight, routed_up_weight, routed_down_weight)
    back = exchange(produced, EP_TP)
    mixer_first_output = project(gathered, mixer_output_weight)
    moe_out = combine(
        back.reshape(experts * 2 * cap, -1), rows, routed_copy_weight.T, shared, cap
    )
    return (mixer_first_output, moe_out)


def solution(mesh):
    split = Mesh(mesh.devices.reshape(4, 4, mesh.shape["tp"]), ("ep_0", "ep_1", "tp"))
    return jax.shard_map(
        on_one,
        mesh=split,
        in_specs=(
            P(EP, "tp"),
            P(EP, "tp"),
            P(EP, "tp"),
            P(EP, "tp"),
            P(EP, "tp"),
            P("tp"),
            P(EP, "tp"),
            P(EP, "tp"),
            P("tp"),
            P(),
            P(EP_TP, None),
            P(),
            P(EP_TP, None),
            P(EP_TP, None),
            P(EP_TP, None, None),
            P(EP_TP, None, None),
            P(EP_TP, None, None),
            P(),
            P(),
            P(),
        ),
        out_specs=(P(EP_TP, None), P(EP_TP, None)),
        check_vma=False,
    )
```

```python
import jax
import jax.numpy as jnp
from jax import lax
from jax.experimental import pallas as pl
from jax.experimental.pallas import tpu as pltpu
from jax.sharding import Mesh
from jax.sharding import PartitionSpec as P


EP = ("ep_0", "ep_1")
EP_TP = ("ep_0", "ep_1", "tp")
BLK = 128
F32 = jnp.float32
BF16 = jnp.bfloat16
NEG = -1e30


def split_two(x):
    hi = x.astype(BF16)
    return hi, (x - hi.astype(F32)).astype(BF16)


def dot(a, b, dims=(((1,), (0,)), ((), ()))):
    return lax.dot_general(a, b, dims, preferred_element_type=F32)


def exact_dot(a, b, dims=(((1,), (0,)), ((), ()))):
    return lax.dot_general(
        a, b, dims, precision=lax.Precision.HIGHEST, preferred_element_type=F32
    )


def iota(shape, dim):
    return lax.broadcasted_iota(jnp.int32, shape, dim)


def whole(shape):
    return pl.BlockSpec(shape, lambda *_: (0,) * len(shape))


def params(mib, grid=False):
    return pltpu.CompilerParams(
        vmem_limit_bytes=mib * 2**20,
        dimension_semantics=("arbitrary",) if grid else None,
    )


def in_hbm(*arrays):
    return [pltpu.with_memory_space_constraint(a, pltpu.HBM) for a in arrays]


def cost(flops, nbytes):
    return pl.CostEstimate(flops=int(flops), bytes_accessed=int(nbytes), transcendentals=0)


def slot_rows(idx, cap, experts):
    tokens = idx.shape[1]
    sub = iota((experts, tokens), 0)
    first = sub == idx[0:1, :]
    second = sub == idx[1:2, :]
    named = jnp.where(first | second, 1.0, 0.0).astype(BF16)
    before = jnp.where(iota((tokens, tokens), 0) < iota((tokens, tokens), 1), 1.0, 0.0)
    prior = dot(named, before.astype(BF16))
    places = [jnp.sum(jnp.where(hot, prior, 0.0), axis=0, keepdims=True) for hot in (first, second)]
    return [
        idx[j : j + 1, :] * (2 * cap) + places[j].astype(jnp.int32) for j in range(2)
    ]


def dispatch_body(cap, experts, x_ref, gain_ref, idx_ref, send_ref, normed_ref, rows_ref, both_ref, want_ref):
    step = pl.program_id(0)
    tokens, width = x_ref.shape
    half = width // 2

    @pl.when(step == 0)
    def _():
        x = x_ref[...].astype(F32)
        scale = lax.rsqrt(jnp.mean(x * x, axis=-1, keepdims=True) + 1e-06)
        normed = (x * scale * gain_ref[...]).astype(BF16)
        normed_ref[...] = normed
        both_ref[0:tokens, :] = normed[:, :half]
        both_ref[tokens:, :] = normed[:, half:]
        row0, row1 = slot_rows(idx_ref[...], cap, experts)
        rows_ref[...] = jnp.concatenate([row0, row1, row0, row1, row0, row1, row0, row1], axis=0)
        want_ref[0:1, 0:tokens] = row0
        want_ref[1:2, 0:tokens] = row1

    rows = send_ref.shape[0]
    row = iota((rows, tokens), 0) + step * rows
    t0, t1 = want_ref[0:1, 0:tokens], want_ref[1:2, 0:tokens]
    low = jnp.where((row == t0) | (row == t1), 1.0, 0.0).astype(BF16)
    high = jnp.where((row == t0 + cap) | (row == t1 + cap), 1.0, 0.0).astype(BF16)
    out = dot(low, both_ref[0:tokens, :]) + dot(high, both_ref[tokens:, :])
    send_ref[...] = out.astype(BF16)


def dispatch_rows(x, gain, idx, cap, experts):
    tokens, width = x.shape
    total = experts * cap * 2
    steps = 4
    body = lambda *refs: dispatch_body(cap, experts, *refs)
    return pl.pallas_call(
        body,
        grid=(steps,),
        in_specs=[whole((tokens, width)), whole((1, width)), whole((2, tokens))],
        out_specs=[
            pl.BlockSpec((total // steps, width // 2), lambda i: (i, 0)),
            whole((tokens, width)),
            whole((8, tokens)),
        ],
        out_shape=[
            pltpu.HBM((total, width // 2), BF16),
            pltpu.HBM((tokens, width), BF16),
            pltpu.HBM((8, tokens), jnp.int32),
        ],
        scratch_shapes=[pltpu.VMEM((2 * tokens, width // 2), BF16), pltpu.VMEM((8, 256), jnp.int32)],
        compiler_params=params(20, True),
        cost_estimate=cost(2 * total * tokens * width, 4 * total * width),
        name="dispatch_rows",
    )(*in_hbm(x, gain, idx))


def swap_halves(even, odd, lower):
    first = jnp.where(lower, even, pltpu.roll(odd, 4, 1))
    last = jnp.where(lower, pltpu.roll(even, 4, 1), odd)
    return first, last


def expert_body(pieces, a_ref, g_hbm, u_hbm, d_hbm, out_hbm, x_ref, h_ref, g_ref, u_ref, d_ref, o_ref, sems):
    pairs = a_ref.shape[0]
    half = a_ref.shape[3]
    hidden = h_ref.shape[1]
    group = 8
    wide = hidden // pieces
    part = half // pieces
    first_loads, last_loads, stores = [], [], []
    for p in range(pieces):
        at = slice(p * wide, (p + 1) * wide)
        first_loads.append(
            [
                pltpu.make_async_copy(g_hbm.at[0, :, at], g_ref.at[p], sems.at[0, p]),
                pltpu.make_async_copy(u_hbm.at[0, :, at], u_ref.at[p], sems.at[1, p]),
            ]
        )
        at = slice(p * part, (p + 1) * part)
        other = slice(half + p * part, half + (p + 1) * part)
        last_loads.append(
            [
                pltpu.make_async_copy(d_hbm.at[0, :, at], d_ref.at[p, 0], sems.at[2, p]),
                pltpu.make_async_copy(d_hbm.at[0, :, other], d_ref.at[p, 1], sems.at[3, p]),
            ]
        )
        stores.append(pltpu.make_async_copy(o_ref.at[p], out_hbm.at[:, :, :, at], sems.at[4, p]))
    loads = first_loads + last_loads
    ahead = 3
    for copies in loads[:ahead]:
        for copy in copies:
            copy.start()
    lower = iota((group, 8, half), 1) < 4
    for i in range(pairs // group):
        tiles = a_ref[i * group : (i + 1) * group].astype(F32)
        first, last = swap_halves(tiles[:, 0], tiles[:, 1], lower)
        at = slice(i * group * 8, (i + 1) * group * 8)
        x_ref[at, 0:half] = first.reshape(group * 8, half).astype(BF16)
        x_ref[at, half:] = last.reshape(group * 8, half).astype(BF16)

    def arrive(n):
        for copy in loads[n]:
            copy.wait()
        if n + ahead < len(loads):
            for copy in loads[n + ahead]:
                copy.start()

    for p in range(pieces):
        arrive(p)
        x = x_ref[...]
        gate = dot(x, g_ref[p])
        up = dot(x, u_ref[p])
        h_ref[:, p * wide : (p + 1) * wide] = (gate * jax.nn.sigmoid(gate) * up).astype(BF16)
    lower = iota((pairs, 8, part), 1) < 4
    for p in range(pieces):
        arrive(pieces + p)
        h = h_ref[...]
        first = dot(h, d_ref[p, 0]).reshape(pairs, 8, part)
        last = dot(h, d_ref[p, 1]).reshape(pairs, 8, part)
        even, odd = swap_halves(first, last, lower)
        o_ref[p, :, 0] = even.astype(BF16)
        o_ref[p, :, 1] = odd.astype(BF16)
        stores[p].start()
    for store in stores:
        store.wait()


def expert_products(arrived, gate_weight, up_weight, down_weight):
    count, rows, half = arrived.shape
    _, width, hidden = gate_weight.shape
    pieces = 4
    shape = (count // 2, 2, rows, half)
    slots = count * rows // 2
    hbm = pl.BlockSpec(memory_space=pltpu.HBM)
    body = lambda *refs: expert_body(pieces, *refs)
    out = pl.pallas_call(
        body,
        in_specs=[pl.BlockSpec(memory_space=pltpu.VMEM), hbm, hbm, hbm],
        out_specs=hbm,
        out_shape=pltpu.HBM(shape, BF16),
        scratch_shapes=[
            pltpu.VMEM((slots, width), BF16),
            pltpu.VMEM((slots, hidden), BF16),
            pltpu.VMEM((pieces, width, hidden // pieces), BF16),
            pltpu.VMEM((pieces, width, hidden // pieces), BF16),
            pltpu.VMEM((pieces, 2, hidden, half // pieces), BF16),
            pltpu.VMEM((pieces, count // 2, 2, rows, half // pieces), BF16),
            pltpu.SemaphoreType.DMA((5, pieces)),
        ],
        compiler_params=params(32),
        cost_estimate=cost(3 * count * rows * width * hidden, 6 * width * hidden),
        name="expert_products",
    )(arrived.reshape(shape), *in_hbm(gate_weight, up_weight, down_weight))
    return out.reshape(arrived.shape)


def shared_body(n_ref, g_ref, u_ref, d_ref, out_ref):
    normed = n_ref[...]
    gate = dot(normed, g_ref[...])
    up = dot(normed, u_ref[...])
    hidden = (gate * jax.nn.sigmoid(gate) * up).astype(BF16)
    out_ref[...] = dot(hidden, d_ref[...])


def shared_expert(normed, gate_weight, up_weight, down_weight):
    tokens, width = normed.shape
    hidden = gate_weight.shape[1]
    return pl.pallas_call(
        shared_body,
        out_shape=pltpu.HBM((tokens, width), F32),
        compiler_params=params(16),
        cost_estimate=cost(6 * tokens * width * hidden, 6 * width * hidden),
        name="shared_expert",
    )(*in_hbm(normed, gate_weight, up_weight, down_weight))


def combine_body(cap, back_ref, rows_ref, weight_ref, shared_hbm, out_hbm, shared_ref, out_ref, sems):
    tokens, _ = out_ref.shape
    total, half = back_ref.shape
    loads, stores = [], []
    for h in range(2):
        cols = slice(h * half, (h + 1) * half)
        loads.append(
            pltpu.make_async_copy(shared_hbm.at[:, cols], shared_ref.at[:, cols], sems.at[0, h])
        )
        stores.append(pltpu.make_async_copy(out_ref.at[:, cols], out_hbm.at[:, cols], sems.at[1, h]))
        loads[h].start()
    row_col = jnp.transpose(rows_ref[...].astype(F32))
    weight_col = jnp.transpose(jnp.concatenate([weight_ref[...]] * 4, axis=0))
    at0, at1 = row_col[:, 0:1].astype(jnp.int32), row_col[:, 1:2].astype(jnp.int32)
    w0, w1 = weight_col[:, 0:1], weight_col[:, 1:2]
    lane = iota((tokens, total), 1)
    for h in range(2):
        cols = slice(h * half, (h + 1) * half)
        mixed = jnp.where(lane == at0 + h * cap, w0, jnp.where(lane == at1 + h * cap, w1, 0.0))
        product = dot(jnp.concatenate(split_two(mixed), axis=0), back_ref[...])
        loads[h].wait()
        routed = product[0:tokens] + product[tokens:]
        out_ref[:, cols] = (routed + shared_ref[:, cols]).astype(BF16)
        stores[h].start()
    for store in stores:
        store.wait()


def combine(back, rows, weights, shared, cap):
    tokens, width = shared.shape
    hbm = pl.BlockSpec(memory_space=pltpu.HBM)
    vmem = pl.BlockSpec(memory_space=pltpu.VMEM)
    body = lambda *refs: combine_body(cap, *refs)
    return pl.pallas_call(
        body,
        in_specs=[vmem, vmem, vmem, hbm],
        out_specs=hbm,
        out_shape=jax.ShapeDtypeStruct((tokens, width), BF16),
        scratch_shapes=[
            pltpu.VMEM((tokens, width), F32),
            pltpu.VMEM((tokens, width), BF16),
            pltpu.SemaphoreType.DMA((2, 2)),
        ],
        compiler_params=params(20),
        cost_estimate=cost(4 * tokens * back.shape[0] * width, 2 * back.size),
        name="combine",
    )(back, rows, weights, *in_hbm(shared))


def gate_rows(in_ref, forget_ref, extra_ref, bias_ref):
    x = forget_ref[...] + bias_ref[0]
    log_forget = jnp.minimum(x, 0.0) - jnp.log1p(jnp.exp(-jnp.abs(x))) + extra_ref[...]
    upper = jnp.where(iota((BLK, BLK), 0) <= iota((BLK, BLK), 1), 1.0, 0.0)
    cumulative = exact_dot(log_forget, upper)
    ones = jnp.ones((BLK, BLK), F32)
    total = exact_dot(log_forget, ones)
    return in_ref[...], cumulative, total


def state_body(k_ref, v_ref, in_ref, forget_ref, extra_ref, bias_ref, out_ref):
    key_dim, length = k_ref.shape
    blocks = length // BLK
    in_gate, cumulative, total = gate_rows(in_ref, forget_ref, extra_ref, bias_ref)
    sums = [jnp.zeros((1, BLK), F32)]
    for j in reversed(range(1, blocks)):
        sums.insert(0, sums[0] + total[j : j + 1, :])
    after = jnp.concatenate(sums, axis=0)
    gap = after + total - cumulative + in_gate
    top = jnp.max(jnp.max(gap, axis=1, keepdims=True), axis=0, keepdims=True)
    weight = jnp.exp(gap - top)
    decay = jnp.sum(total[:, 0:1], axis=0, keepdims=True)
    acc = jnp.zeros((2 * key_dim, 2 * BLK), F32)
    ones = jnp.ones((2 * BLK, BLK), BF16)
    for j in range(blocks // 2):
        at = slice(j * 2 * BLK, (j + 1) * 2 * BLK)
        weights = jnp.concatenate([weight[2 * j : 2 * j + 1], weight[2 * j + 1 : 2 * j + 2]], axis=1)
        keys = k_ref[:, at].astype(F32) * weights
        hi, lo = split_two(keys)
        values = jnp.concatenate([v_ref[at, :], ones], axis=1)
        acc = acc + dot(jnp.concatenate([hi, lo], axis=0), values)
    state = acc[:key_dim] + acc[key_dim:]
    norm = jnp.transpose(state[:, BLK:])[0:8, :]
    norm = jnp.concatenate([norm, jnp.zeros((8, BLK - key_dim), F32)], axis=1)
    lane = iota((8, BLK), 1)
    tail = jnp.where(lane < key_dim, norm, jnp.where(lane < key_dim + 32, top, decay))
    out_ref[0:key_dim, :] = state[:, 0:BLK]
    out_ref[key_dim:, :] = tail


def device_state(keys, values, in_gate, forget, extra, bias):
    key_dim, length = keys.shape
    return pl.pallas_call(
        state_body,
        in_specs=[pl.BlockSpec(memory_space=pltpu.VMEM)] * 5 + [pl.BlockSpec(memory_space=pltpu.SMEM)],
        out_shape=jax.ShapeDtypeStruct((key_dim + 8, BLK), F32),
        compiler_params=params(8),
        cost_estimate=cost(8 * length * key_dim * BLK, 4 * length * BLK),
        name="device_state",
    )(*in_hbm(keys, values, in_gate, forget, extra), bias)


def incoming_state(place, states, key_dim):
    since = jnp.zeros((1, 1), F32)
    gaps, counted = [], []
    top = jnp.full((1, 1), NEG, F32)
    for k, ref in enumerate(states, 1):
        tail = ref[key_dim : key_dim + 1, :]
        counted.append(jnp.full((1, 1), k, jnp.int32) <= place)
        gaps.append(jnp.where(counted[-1], tail[:, key_dim : key_dim + 1] + since, NEG))
        since = since + tail[:, key_dim + 32 : key_dim + 33]
        top = jnp.maximum(top, gaps[-1])
    memory = jnp.zeros((key_dim + 8, BLK), F32)
    for ref, gap, c in zip(states, gaps, counted):
        memory = memory + ref[...] * jnp.where(c, jnp.exp(gap - top), 0.0)
    norm = jnp.broadcast_to(memory[key_dim : key_dim + 1, :], (BLK, BLK))
    norm = jnp.transpose(norm)[0:key_dim, :]
    return jnp.concatenate([memory[0:key_dim], norm], axis=1), top


def mixer_body(
    state_count,
    place_ref,
    bias_ref,
    q_ref,
    k_ref,
    v_ref,
    in_ref,
    forget_ref,
    extra_ref,
    gate_ref,
    gain_ref,
    *refs,
):
    key_dim, length = k_ref.shape
    blocks = length // BLK
    states = refs[:state_count]
    *outs, out_ref = refs[state_count:]
    peers = len(outs)
    tokens = length // peers
    per_chunk = tokens // BLK
    in_gate, cumulative, total = gate_rows(in_ref, forget_ref, extra_ref, bias_ref)
    state, top = incoming_state(place_ref[0], states, key_dim)
    gap = total - cumulative + in_gate
    block_top = jnp.max(gap, axis=1, keepdims=True)
    weight = jnp.exp(gap - block_top)
    shifted = in_gate - cumulative
    sum_col = jnp.transpose(jnp.concatenate([cumulative] * (BLK // blocks), axis=0))
    ones = jnp.ones((BLK, BLK), BF16)
    lower = iota((BLK, BLK), 1) <= iota((BLK, BLK), 0)
    gain = gain_ref[...]
    eight = jnp.ones((8, BLK), F32)
    squares = []
    for j in range(blocks):
        at = slice(j * BLK, (j + 1) * BLK)
        keys = k_ref[:, at]
        values = jnp.concatenate([v_ref[at, :], ones], axis=1)
        query = jnp.transpose(q_ref[:, at].astype(F32) * (key_dim**-0.5)).astype(BF16)
        base = sum_col[:, j : j + 1]
        pair = jnp.where(lower, base + shifted[j : j + 1, :], -jnp.inf)
        carried = base + top
        stable = jnp.maximum(carried, jnp.max(pair, axis=1, keepdims=True))
        scores = dot(query, keys) * jnp.exp(pair - stable)
        carry = jnp.exp(carried - stable)
        score_hi, score_lo = split_two(scores)
        state_hi, state_lo = split_two(state)
        both = dot(score_hi, values) + dot(score_lo, values)
        both = both + carry * (dot(query, state_hi) + dot(query, state_lo))
        hidden = both[:, :BLK] / jnp.maximum(jnp.abs(both[:, BLK:]), jnp.exp(-stable))
        squares.append(
            exact_dot(eight, hidden * hidden, (((1,), (1,)), ((), ())))[0:1, :]
        )
        gated = hidden * gain * jax.nn.sigmoid(gate_ref[at, :].astype(F32))
        start = (j % per_chunk) * BLK
        out_ref[j // per_chunk, start : start + BLK, :] = gated.astype(BF16)
        if j + 1 < blocks:
            hi, lo = split_two(keys.astype(F32) * weight[j : j + 1, :])
            added = dot(jnp.concatenate([hi, lo], axis=0), values)
            added = added[:key_dim] + added[key_dim:]
            late = block_top[j : j + 1, :]
            early = total[j : j + 1, 0:1] + top
            top = jnp.maximum(early, late)
            state = jnp.exp(early - top) * state + jnp.exp(late - top) * added
    for c in range(peers):
        own = squares[c * per_chunk : (c + 1) * per_chunk]
        parts = [split_two(row) for row in own]
        rows = [hi.astype(F32) for hi, _ in parts] + [lo.astype(F32) for _, lo in parts]
        rows.append(jnp.zeros((16 - len(rows), BLK), F32))
        out_ref[c, tokens:, :] = jnp.concatenate(rows, axis=0).astype(BF16)
    for k in range(peers):
        outs[k][...] = out_ref[(place_ref[1] + k) % peers]


def mixer_rows(place, bias, states, queries, keys, values, in_gate, forget, extra, gate, gain, peers):
    _, length = keys.shape
    smem = pl.BlockSpec(memory_space=pltpu.SMEM)
    vmem = pl.BlockSpec(memory_space=pltpu.VMEM)
    chunk = (length // peers + 16, BLK)
    body = lambda *refs: mixer_body(len(states), *refs)
    return pl.pallas_call(
        body,
        in_specs=[smem, smem] + [vmem] * (8 + len(states)),
        out_shape=[jax.ShapeDtypeStruct(chunk, BF16)] * peers,
        scratch_shapes=[pltpu.VMEM((peers, *chunk), BF16)],
        compiler_params=params(16),
        cost_estimate=cost(32 * length * BLK * BLK, 8 * length * BLK),
        name="mixer_rows",
    )(
        place,
        bias,
        *in_hbm(queries, keys, values, in_gate, forget, extra, gate, gain),
        *states,
    )


def project_body(heads, place_ref, *refs):
    chunks = refs[:heads]
    w_ref, out_ref, all_ref, scale_ref = refs[heads:]
    tokens = out_ref.shape[0]
    per_chunk = tokens // BLK

    @pl.when(pl.program_id(0) == 0)
    def _():
        tail = chunks[0][tokens:, :].astype(F32)
        for k in range(1, heads):
            tail = tail + chunks[k][tokens:, :].astype(F32)
        for c in range(per_chunk):
            row = tail[c : c + 1, :] + tail[per_chunk + c : per_chunk + c + 1, :]
            row = lax.rsqrt(row / (heads * BLK) + 1e-06)
            scale_ref[c * BLK : (c + 1) * BLK, :] = jnp.transpose(jnp.broadcast_to(row, (BLK, BLK)))
        for k in range(heads):
            all_ref[(place_ref[1] + heads - k) % heads] = chunks[k][0:tokens, :]

    mixed = jnp.concatenate([all_ref[h] for h in range(heads)], axis=1)
    product = dot(mixed, w_ref[...])
    out_ref[...] = (product * scale_ref[:, 0:1]).astype(BF16)


def project(place, chunks, weight):
    heads = len(chunks)
    rows = chunks[0].shape[0]
    tokens = rows - 16
    width = weight.shape[1]
    steps = 4
    body = lambda *refs: project_body(heads, *refs)
    return pl.pallas_call(
        body,
        grid=(steps,),
        in_specs=[pl.BlockSpec(memory_space=pltpu.SMEM)]
        + [whole((rows, BLK))] * heads
        + [pl.BlockSpec((weight.shape[0], width // steps), lambda i: (0, i))],
        out_specs=pl.BlockSpec((tokens, width // steps), lambda i: (0, i)),
        out_shape=jax.ShapeDtypeStruct((tokens, width), BF16),
        scratch_shapes=[pltpu.VMEM((heads, tokens, BLK), BF16), pltpu.VMEM((tokens, BLK), F32)],
        compiler_params=params(16, True),
        cost_estimate=cost(2 * tokens * weight.size, 2 * weight.size),
        name="project",
    )(place, *chunks, *in_hbm(weight))


def exchange(x, axes):
    return lax.all_to_all(x, axes, split_axis=0, concat_axis=0, tiled=True)


def from_earlier(shards, axes, wrap):
    count = lax.axis_size(axes)
    return [
        lax.ppermute(
            shard, axes, [(p, (p + k) % count) for p in range(count if wrap else count - k)]
        )
        for k, shard in enumerate(shards, 1)
    ]


def on_one(
    queries,
    head_key_rows,
    head_value_rows,
    log_input_gate,
    forget_logits,
    head_forget_bias,
    extra_log_forget,
    output_gate_logits,
    head_norm_gain,
    mixer_output_weight,
    second_batch_input,
    expert_norm_gain,
    routed_expert_index,
    routed_copy_weight,
    routed_gate_weight,
    routed_up_weight,
    routed_down_weight,
    shared_gate_weight,
    shared_up_weight,
    shared_down_weight,
):
    length = queries.shape[0]
    ep_count, tp_count = lax.axis_size(EP), lax.axis_size("tp")
    experts = ep_count * tp_count
    cap = 4
    send, normed, rows = dispatch_rows(
        second_batch_input, expert_norm_gain[None, :], routed_expert_index.T, cap, experts
    )
    landed = exchange(send.reshape(experts, 2 * cap, -1), EP_TP)

    def by_block(a):
        return a.reshape(length // BLK, BLK)

    in_gate, forget, extra = (
        by_block(log_input_gate),
        by_block(forget_logits),
        by_block(extra_log_forget),
    )
    query_rows, key_rows = queries.T, head_key_rows.T
    place = jnp.stack([lax.axis_index(a).astype(jnp.int32) for a in (EP, "tp")])
    own = device_state(key_rows, head_value_rows, in_gate, forget, extra, head_forget_bias)
    states = from_earlier([own] * (ep_count - 1), EP, False)
    chunks = mixer_rows(
        place,
        head_forget_bias,
        states,
        query_rows,
        key_rows,
        head_value_rows,
        in_gate,
        forget,
        extra,
        output_gate_logits,
        head_norm_gain[None, :],
        tp_count,
    )
    shared = shared_expert(normed, shared_gate_weight, shared_up_weight, shared_down_weight)
    gathered = [chunks[0]] + from_earlier(chunks[1:], "tp", True)
    produced = expert_products(landed, routed_gate_weight, routed_up_weight, routed_down_weight)
    back = exchange(produced, EP_TP)
    mixer_first_output = project(place, gathered, mixer_output_weight)
    moe_out = combine(
        back.reshape(experts * 2 * cap, -1), rows, routed_copy_weight.T, shared, cap
    )
    return (mixer_first_output, moe_out)


def solution(mesh):
    split = Mesh(mesh.devices.reshape(4, 4, mesh.shape["tp"]), ("ep_0", "ep_1", "tp"))
    return jax.shard_map(
        on_one,
        mesh=split,
        in_specs=(
            P(EP, "tp"),
            P(EP, "tp"),
            P(EP, "tp"),
            P(EP, "tp"),
            P(EP, "tp"),
            P("tp"),
            P(EP, "tp"),
            P(EP, "tp"),
            P("tp"),
            P(),
            P(EP_TP, None),
            P(),
            P(EP_TP, None),
            P(EP_TP, None),
            P(EP_TP, None, None),
            P(EP_TP, None, None),
            P(EP_TP, None, None),
            P(),
            P(),
            P(),
        ),
        out_specs=(P(EP_TP, None), P(EP_TP, None)),
        check_vma=False,
    )
```

```python
import jax
import jax.numpy as jnp
from jax import lax
from jax.experimental import pallas as pl
from jax.experimental.pallas import tpu as pltpu
from jax.sharding import Mesh
from jax.sharding import PartitionSpec as P


EP = ("ep_0", "ep_1")
EP_TP = ("ep_0", "ep_1", "tp")
BLK = 128
F32 = jnp.float32
BF16 = jnp.bfloat16
NEG = -1e30


def split_two(x):
    hi = x.astype(BF16)
    return hi, (x - hi.astype(F32)).astype(BF16)


def dot(a, b, dims=(((1,), (0,)), ((), ()))):
    return lax.dot_general(a, b, dims, preferred_element_type=F32)


def exact_dot(a, b, dims=(((1,), (0,)), ((), ()))):
    return lax.dot_general(
        a, b, dims, precision=lax.Precision.HIGHEST, preferred_element_type=F32
    )


def iota(shape, dim):
    return lax.broadcasted_iota(jnp.int32, shape, dim)


def params(mib, grid=False):
    return pltpu.CompilerParams(
        vmem_limit_bytes=mib * 2**20,
        dimension_semantics=("arbitrary",) if grid else None,
    )


def in_hbm(*arrays):
    return [pltpu.with_memory_space_constraint(a, pltpu.HBM) for a in arrays]


def cost(flops, nbytes):
    return pl.CostEstimate(flops=int(flops), bytes_accessed=int(nbytes), transcendentals=0)


def copy_slots(idx, cap, experts):
    tokens = idx.shape[1]
    sub = iota((experts, tokens), 0)
    first = sub == idx[0:1, :]
    second = sub == idx[1:2, :]
    named = jnp.where(first | second, 1.0, 0.0).astype(BF16)
    before = jnp.where(iota((tokens, tokens), 0) < iota((tokens, tokens), 1), 1.0, 0.0)
    prior = dot(named, before.astype(BF16))
    places = [jnp.sum(jnp.where(hot, prior, 0.0), axis=0, keepdims=True) for hot in (first, second)]
    return [idx[j : j + 1, :] * cap + places[j].astype(jnp.int32) for j in range(2)]


def dispatch_body(
    cap, x_hbm, gain_hbm, idx_hbm, send_hbm, normed_hbm, slots_hbm,
    x_ref, gain_ref, idx_ref, send_ref, normed_ref, slots_ref, in_sems, out_sems,
):
    tokens, width = x_ref.shape
    half = width // 2
    pieces, pairs = send_ref.shape[0:2]
    experts = 2 * pieces * pairs
    loads = [
        pltpu.make_async_copy(src, dst, in_sems.at[i])
        for i, (src, dst) in enumerate(((idx_hbm, idx_ref), (gain_hbm, gain_ref), (x_hbm, x_ref)))
    ]
    for load in loads:
        load.start()
    loads[0].wait()
    slot0, slot1 = copy_slots(idx_ref[...], cap, experts)
    slots_ref[...] = jnp.concatenate([slot0, slot1] * 4, axis=0)
    stores = [pltpu.make_async_copy(slots_ref, slots_hbm, out_sems.at[pieces])]
    stores[0].start()
    loads[1].wait()
    loads[2].wait()
    x = x_ref[...].astype(F32)
    scale = lax.rsqrt(jnp.mean(x * x, axis=-1, keepdims=True) + 1e-06)
    normed = (x * scale * gain_ref[...]).astype(BF16)
    normed_ref[...] = normed
    lower = iota((pairs, 8, half), 1) < 4
    rows = pairs * 2 * cap
    for p in range(pieces):
        row = iota((rows, tokens), 0) + p * rows
        wanted = jnp.where((row == slot0) | (row == slot1), 1.0, 0.0).astype(BF16)
        first = dot(wanted, normed_ref[:, :half]).reshape(pairs, 8, half)
        last = dot(wanted, normed_ref[:, half:]).reshape(pairs, 8, half)
        even, odd = swap_halves(first, last, lower)
        send_ref[p, :, 0] = even.astype(BF16)
        send_ref[p, :, 1] = odd.astype(BF16)
        stores.append(pltpu.make_async_copy(send_ref.at[p], send_hbm.at[p], out_sems.at[p]))
        stores[-1].start()
    stores.append(pltpu.make_async_copy(normed_ref, normed_hbm, out_sems.at[pieces + 1]))
    stores[-1].start()
    for store in stores:
        store.wait()


def dispatch_rows(x, gain, idx, cap, experts):
    tokens, width = x.shape
    pieces = 4
    shape = (pieces, experts // (2 * pieces), 2, 2 * cap, width // 2)
    hbm = pl.BlockSpec(memory_space=pltpu.HBM)
    body = lambda *refs: dispatch_body(cap, *refs)
    return pl.pallas_call(
        body,
        in_specs=[hbm] * 3,
        out_specs=[hbm] * 3,
        out_shape=[
            pltpu.HBM(shape, BF16),
            pltpu.HBM((tokens, width), BF16),
            pltpu.HBM((8, tokens), jnp.int32),
        ],
        scratch_shapes=[
            pltpu.VMEM((tokens, width), BF16),
            pltpu.VMEM((1, width), F32),
            pltpu.VMEM((2, tokens), jnp.int32),
            pltpu.VMEM(shape, BF16),
            pltpu.VMEM((tokens, width), BF16),
            pltpu.VMEM((8, tokens), jnp.int32),
            pltpu.SemaphoreType.DMA((3,)),
            pltpu.SemaphoreType.DMA((pieces + 2,)),
        ],
        compiler_params=params(20),
        cost_estimate=cost(2 * experts * cap * tokens * width, 4 * experts * cap * width),
        name="dispatch_rows",
    )(*in_hbm(x, gain, idx))


def swap_halves(even, odd, lower):
    first = jnp.where(lower, even, pltpu.roll(odd, 4, 1))
    last = jnp.where(lower, pltpu.roll(even, 4, 1), odd)
    return first, last


def expert_body(pieces, a_ref, g_hbm, u_hbm, d_hbm, out_hbm, x_ref, h_ref, g_ref, u_ref, d_ref, o_ref, sems):
    pairs = a_ref.shape[0]
    half = a_ref.shape[3]
    hidden = h_ref.shape[1]
    group = 8
    wide = hidden // pieces
    part = half // pieces
    first_loads, last_loads, stores = [], [], []
    for p in range(pieces):
        at = slice(p * wide, (p + 1) * wide)
        first_loads.append(
            [
                pltpu.make_async_copy(g_hbm.at[0, :, at], g_ref.at[p], sems.at[0, p]),
                pltpu.make_async_copy(u_hbm.at[0, :, at], u_ref.at[p], sems.at[1, p]),
            ]
        )
        at = slice(p * part, (p + 1) * part)
        other = slice(half + p * part, half + (p + 1) * part)
        last_loads.append(
            [
                pltpu.make_async_copy(d_hbm.at[0, :, at], d_ref.at[p, 0], sems.at[2, p]),
                pltpu.make_async_copy(d_hbm.at[0, :, other], d_ref.at[p, 1], sems.at[3, p]),
            ]
        )
        stores.append(pltpu.make_async_copy(o_ref.at[p], out_hbm.at[:, :, :, at], sems.at[4, p]))
    for copies in first_loads + last_loads:
        for copy in copies:
            copy.start()
    lower = iota((group, 8, half), 1) < 4
    for i in range(pairs // group):
        tiles = a_ref[i * group : (i + 1) * group].astype(F32)
        first, last = swap_halves(tiles[:, 0], tiles[:, 1], lower)
        at = slice(i * group * 8, (i + 1) * group * 8)
        x_ref[at, 0:half] = first.reshape(group * 8, half).astype(BF16)
        x_ref[at, half:] = last.reshape(group * 8, half).astype(BF16)

    for p in range(pieces):
        for copy in first_loads[p]:
            copy.wait()
        x = x_ref[...]
        gate = dot(x, g_ref[p])
        up = dot(x, u_ref[p])
        h_ref[:, p * wide : (p + 1) * wide] = (gate * jax.nn.sigmoid(gate) * up).astype(BF16)
    lower = iota((pairs, 8, part), 1) < 4
    for p in range(pieces):
        for copy in last_loads[p]:
            copy.wait()
        h = h_ref[...]
        first = dot(h, d_ref[p, 0]).reshape(pairs, 8, part)
        last = dot(h, d_ref[p, 1]).reshape(pairs, 8, part)
        even, odd = swap_halves(first, last, lower)
        o_ref[p, :, 0] = even.astype(BF16)
        o_ref[p, :, 1] = odd.astype(BF16)
        stores[p].start()
    for store in stores:
        store.wait()


def expert_products(arrived, gate_weight, up_weight, down_weight):
    count, rows, half = arrived.shape
    _, width, hidden = gate_weight.shape
    pieces = 4
    shape = (count // 2, 2, rows, half)
    slots = count * rows // 2
    hbm = pl.BlockSpec(memory_space=pltpu.HBM)
    body = lambda *refs: expert_body(pieces, *refs)
    out = pl.pallas_call(
        body,
        in_specs=[pl.BlockSpec(memory_space=pltpu.VMEM), hbm, hbm, hbm],
        out_specs=hbm,
        out_shape=pltpu.HBM(shape, BF16),
        scratch_shapes=[
            pltpu.VMEM((slots, width), BF16),
            pltpu.VMEM((slots, hidden), BF16),
            pltpu.VMEM((pieces, width, hidden // pieces), BF16),
            pltpu.VMEM((pieces, width, hidden // pieces), BF16),
            pltpu.VMEM((pieces, 2, hidden, half // pieces), BF16),
            pltpu.VMEM((pieces, count // 2, 2, rows, half // pieces), BF16),
            pltpu.SemaphoreType.DMA((5, pieces)),
        ],
        compiler_params=params(32),
        cost_estimate=cost(3 * count * rows * width * hidden, 6 * width * hidden),
        name="expert_products",
    )(arrived.reshape(shape), *in_hbm(gate_weight, up_weight, down_weight))
    return out.reshape(arrived.shape)


def shared_body(n_ref, g_ref, u_ref, d_ref, out_ref):
    normed = n_ref[...]
    gate = dot(normed, g_ref[...])
    up = dot(normed, u_ref[...])
    hidden = (gate * jax.nn.sigmoid(gate) * up).astype(BF16)
    out_ref[...] = dot(hidden, d_ref[...])


def shared_expert(normed, gate_weight, up_weight, down_weight):
    tokens, width = normed.shape
    hidden = gate_weight.shape[1]
    return pl.pallas_call(
        shared_body,
        out_shape=pltpu.HBM((tokens, width), F32),
        compiler_params=params(16),
        cost_estimate=cost(6 * tokens * width * hidden, 6 * width * hidden),
        name="shared_expert",
    )(*in_hbm(normed, gate_weight, up_weight, down_weight))


def combine_body(
    cap, back_ref, slots_ref, weight_ref, shared_hbm, w_hbm, out_hbm, w_ref, shared_ref, out_ref, sems, w_sem
):
    tokens, _ = out_ref.shape
    total, half = back_ref.shape
    loads, stores = [], []
    for h in range(2):
        cols = slice(h * half, (h + 1) * half)
        loads.append(
            pltpu.make_async_copy(shared_hbm.at[:, cols], shared_ref.at[:, cols], sems.at[0, h])
        )
        stores.append(pltpu.make_async_copy(out_ref.at[:, cols], out_hbm.at[:, cols], sems.at[1, h]))
        loads[h].start()
    bring = pltpu.make_async_copy(w_hbm, w_ref, w_sem)
    bring.start()
    slot_col = jnp.transpose(slots_ref[...].astype(F32)).astype(jnp.int32)
    weight_col = jnp.transpose(jnp.concatenate([weight_ref[...]] * 4, axis=0)).astype(BF16)
    lane = iota((tokens, total), 1)
    at = [(s // cap) * (2 * cap) + s % cap for s in (slot_col[:, 0:1], slot_col[:, 1:2])]
    for h in range(2):
        cols = slice(h * half, (h + 1) * half)
        mix = jnp.where(
            lane == at[0] + h * cap,
            weight_col[:, 0:1].astype(F32),
            jnp.where(lane == at[1] + h * cap, weight_col[:, 1:2].astype(F32), 0.0),
        ).astype(BF16)
        routed = dot(mix, back_ref[...])
        loads[h].wait()
        out_ref[:, cols] = (routed + shared_ref[:, cols]).astype(BF16)
        stores[h].start()
    for store in stores:
        store.wait()
    bring.wait()


def combine(back, slots, weights, shared, cap, mixer_weight):
    tokens, width = shared.shape
    hbm = pl.BlockSpec(memory_space=pltpu.HBM)
    vmem = pl.BlockSpec(memory_space=pltpu.VMEM)
    body = lambda *refs: combine_body(cap, *refs)
    return pl.pallas_call(
        body,
        in_specs=[vmem, vmem, vmem, hbm, hbm],
        out_specs=[hbm, vmem],
        out_shape=[
            jax.ShapeDtypeStruct((tokens, width), BF16),
            pltpu.VMEM(mixer_weight.shape, BF16),
        ],
        scratch_shapes=[
            pltpu.VMEM((tokens, width), F32),
            pltpu.VMEM((tokens, width), BF16),
            pltpu.SemaphoreType.DMA((2, 2)),
            pltpu.SemaphoreType.DMA,
        ],
        compiler_params=params(20),
        cost_estimate=cost(4 * tokens * back.shape[0] * width, 2 * back.size),
        name="combine",
    )(back, slots, weights, *in_hbm(shared, mixer_weight))


def gate_rows(in_ref, forget_ref, extra_ref, bias_ref):
    x = forget_ref[...] + bias_ref[0]
    log_forget = jnp.minimum(x, 0.0) - jnp.log1p(jnp.exp(-jnp.abs(x))) + extra_ref[...]
    upper = jnp.where(iota((BLK, BLK), 0) <= iota((BLK, BLK), 1), 1.0, 0.0)
    cumulative = exact_dot(log_forget, upper)
    ones = jnp.ones((BLK, BLK), F32)
    total = exact_dot(log_forget, ones)
    return in_ref[...], cumulative, total


def state_body(k_ref, v_ref, in_ref, forget_ref, extra_ref, bias_ref, out_ref):
    key_dim, length = k_ref.shape
    blocks = length // BLK
    in_gate, cumulative, total = gate_rows(in_ref, forget_ref, extra_ref, bias_ref)
    sums = [jnp.zeros((1, BLK), F32)]
    for j in reversed(range(1, blocks)):
        sums.insert(0, sums[0] + total[j : j + 1, :])
    after = jnp.concatenate(sums, axis=0)
    gap = after + total - cumulative + in_gate
    top = jnp.max(jnp.max(gap, axis=1, keepdims=True), axis=0, keepdims=True)
    weight = jnp.exp(gap - top)
    decay = jnp.sum(total[:, 0:1], axis=0, keepdims=True)
    acc = jnp.zeros((2 * key_dim, 2 * BLK), F32)
    ones = jnp.ones((2 * BLK, BLK), BF16)
    for j in range(blocks // 2):
        at = slice(j * 2 * BLK, (j + 1) * 2 * BLK)
        weights = jnp.concatenate([weight[2 * j : 2 * j + 1], weight[2 * j + 1 : 2 * j + 2]], axis=1)
        keys = k_ref[:, at].astype(F32) * weights
        hi, lo = split_two(keys)
        values = jnp.concatenate([v_ref[at, :], ones], axis=1)
        acc = acc + dot(jnp.concatenate([hi, lo], axis=0), values)
    state = acc[:key_dim] + acc[key_dim:]
    norm = jnp.transpose(state[:, BLK:])[0:8, :]
    norm = jnp.concatenate([norm, jnp.zeros((8, BLK - key_dim), F32)], axis=1)
    lane = iota((8, BLK), 1)
    tail = jnp.where(lane < key_dim, norm, jnp.where(lane < key_dim + 32, top, decay))
    out_ref[0:key_dim, :] = state[:, 0:BLK]
    out_ref[key_dim:, :] = tail


def device_state(keys, values, in_gate, forget, extra, bias):
    key_dim, length = keys.shape
    return pl.pallas_call(
        state_body,
        in_specs=[pl.BlockSpec(memory_space=pltpu.VMEM)] * 5 + [pl.BlockSpec(memory_space=pltpu.SMEM)],
        out_shape=jax.ShapeDtypeStruct((key_dim + 8, BLK), F32),
        compiler_params=params(8),
        cost_estimate=cost(8 * length * key_dim * BLK, 4 * length * BLK),
        name="device_state",
    )(*in_hbm(keys, values, in_gate, forget, extra), bias)


def merge_states(refs, keys, counted, key_dim):
    tails = [ref[key_dim : key_dim + 1, :] for ref in refs]
    tops = [t[:, key_dim : key_dim + 1] for t in tails]
    decays = [
        jnp.where(c, t[:, key_dim + 32 : key_dim + 33], 0.0) for t, c in zip(tails, counted)
    ]
    gaps = []
    for i, key in enumerate(keys):
        since = jnp.zeros((1, 1), F32)
        for j, other in enumerate(keys):
            if j != i:
                since = since + jnp.where(other > key, decays[j], 0.0)
        gaps.append(jnp.where(counted[i], tops[i] + since, NEG))
    top = gaps[0]
    for gap in gaps[1:]:
        top = jnp.maximum(top, gap)
    merged = jnp.zeros((key_dim + 8, BLK), F32)
    for ref, gap, c in zip(refs, gaps, counted):
        merged = merged + ref[...] * jnp.where(c, jnp.exp(gap - top), 0.0)
    return merged, top, sum(decays)


def as_one(scalar):
    return jnp.full((1, 1), scalar, jnp.int32)


def ring_places(place, count):
    return [as_one((place + count - k) % count) for k in range(count)]


def row_body(place_ref, *refs):
    *states, out_ref = refs
    key_dim = out_ref.shape[0] - 8
    keys = ring_places(place_ref[1], len(states))
    counted = [jnp.full((1, 1), True)] * len(states)
    merged, top, decay = merge_states(states, keys, counted, key_dim)
    lane = iota((8, BLK), 1)
    norm = merged[key_dim:, :]
    out_ref[0:key_dim, :] = merged[0:key_dim]
    out_ref[key_dim:, :] = jnp.where(
        lane < key_dim, norm, jnp.where(lane < key_dim + 32, top, decay)
    )


def row_state(place, states):
    return pl.pallas_call(
        row_body,
        in_specs=[pl.BlockSpec(memory_space=pltpu.SMEM)]
        + [pl.BlockSpec(memory_space=pltpu.VMEM)] * len(states),
        out_shape=jax.ShapeDtypeStruct(states[0].shape, F32),
        compiler_params=params(4),
        cost_estimate=cost(2**20, 2**18),
        name="row_state",
    )(place, *states)


def incoming_state(place_ref, rows, columns, key_dim):
    in_row = ring_places(place_ref[1], len(rows))
    in_column = ring_places(place_ref[0], len(columns) + 1)[1:]
    counted = [p < as_one(place_ref[1]) for p in in_row[1:]]
    counted += [p < as_one(place_ref[0]) for p in in_column]
    keys = [p + len(columns) + 1 for p in in_row[1:]] + in_column
    memory, top, _ = merge_states(rows[1:] + columns, keys, counted, key_dim)
    norm = jnp.broadcast_to(memory[key_dim : key_dim + 1, :], (BLK, BLK))
    norm = jnp.transpose(norm)[0:key_dim, :]
    return jnp.concatenate([memory[0:key_dim], norm], axis=1), top


def mixer_body(
    rows_count,
    columns_count,
    place_ref,
    bias_ref,
    q_ref,
    k_ref,
    v_ref,
    in_ref,
    forget_ref,
    extra_ref,
    gate_ref,
    gain_ref,
    *refs,
):
    key_dim, length = k_ref.shape
    blocks = length // BLK
    rows = list(refs[:rows_count])
    columns = list(refs[rows_count : rows_count + columns_count])
    *outs, out_ref = refs[rows_count + columns_count :]
    peers = len(outs)
    tokens = length // peers
    per_chunk = tokens // BLK
    in_gate, cumulative, total = gate_rows(in_ref, forget_ref, extra_ref, bias_ref)
    state, top = incoming_state(place_ref, rows, columns, key_dim)
    gap = total - cumulative + in_gate
    block_top = jnp.max(gap, axis=1, keepdims=True)
    weight = jnp.exp(gap - block_top)
    shifted = in_gate - cumulative
    sum_col = jnp.transpose(jnp.concatenate([cumulative] * (BLK // blocks), axis=0))
    ones = jnp.ones((BLK, BLK), BF16)
    lower = iota((BLK, BLK), 1) <= iota((BLK, BLK), 0)
    gain = gain_ref[...]
    eight = jnp.ones((8, BLK), F32)
    squares = []
    for j in range(blocks):
        at = slice(j * BLK, (j + 1) * BLK)
        keys = k_ref[:, at]
        values = jnp.concatenate([v_ref[at, :], ones], axis=1)
        query = jnp.transpose(q_ref[:, at].astype(F32) * (key_dim**-0.5)).astype(BF16)
        base = sum_col[:, j : j + 1]
        pair = jnp.where(lower, base + shifted[j : j + 1, :], -jnp.inf)
        carried = base + top
        stable = jnp.maximum(carried, jnp.max(pair, axis=1, keepdims=True))
        scores = dot(query, keys) * jnp.exp(pair - stable)
        carry = jnp.exp(carried - stable)
        score_hi, score_lo = split_two(scores)
        state_hi, state_lo = split_two(state)
        both = dot(score_hi, values) + dot(score_lo, values)
        both = both + carry * (dot(query, state_hi) + dot(query, state_lo))
        hidden = both[:, :BLK] / jnp.maximum(jnp.abs(both[:, BLK:]), jnp.exp(-stable))
        squares.append(
            exact_dot(eight, hidden * hidden, (((1,), (1,)), ((), ())))[0:1, :]
        )
        gated = hidden * gain * jax.nn.sigmoid(gate_ref[at, :].astype(F32))
        start = (j % per_chunk) * BLK
        out_ref[j // per_chunk, start : start + BLK, :] = gated.astype(BF16)
        if j + 1 < blocks:
            hi, lo = split_two(keys.astype(F32) * weight[j : j + 1, :])
            added = dot(jnp.concatenate([hi, lo], axis=0), values)
            added = added[:key_dim] + added[key_dim:]
            late = block_top[j : j + 1, :]
            early = total[j : j + 1, 0:1] + top
            top = jnp.maximum(early, late)
            state = jnp.exp(early - top) * state + jnp.exp(late - top) * added
    for c in range(peers):
        own = squares[c * per_chunk : (c + 1) * per_chunk]
        parts = [split_two(row) for row in own]
        rows = [hi.astype(F32) for hi, _ in parts] + [lo.astype(F32) for _, lo in parts]
        rows.append(jnp.zeros((16 - len(rows), BLK), F32))
        out_ref[c, tokens:, :] = jnp.concatenate(rows, axis=0).astype(BF16)
    for k in range(peers):
        outs[k][...] = out_ref[(place_ref[2] + k) % peers]


def mixer_rows(place, bias, rows, columns, queries, keys, values, in_gate, forget, extra, gate, gain, peers):
    _, length = keys.shape
    smem = pl.BlockSpec(memory_space=pltpu.SMEM)
    vmem = pl.BlockSpec(memory_space=pltpu.VMEM)
    chunk = (length // peers + 16, BLK)
    body = lambda *refs: mixer_body(len(rows), len(columns), *refs)
    return pl.pallas_call(
        body,
        in_specs=[smem, smem] + [vmem] * (8 + len(rows) + len(columns)),
        out_shape=[jax.ShapeDtypeStruct(chunk, BF16)] * peers,
        scratch_shapes=[pltpu.VMEM((peers, *chunk), BF16)],
        compiler_params=params(16),
        cost_estimate=cost(32 * length * BLK * BLK, 8 * length * BLK),
        name="mixer_rows",
    )(
        place,
        bias,
        *in_hbm(queries, keys, values, in_gate, forget, extra, gate, gain),
        *rows,
        *columns,
    )


def project_body(heads, place_ref, *refs):
    chunks = refs[:heads]
    w_ref, out_hbm, all_ref, out_ref, sems = refs[heads:]
    pieces, tokens, wide = out_ref.shape
    per_chunk = tokens // BLK
    for k in range(heads):
        all_ref[(place_ref[2] + heads - k) % heads] = chunks[k][0:tokens, :]
    tail = chunks[0][tokens:, :].astype(F32)
    for k in range(1, heads):
        tail = tail + chunks[k][tokens:, :].astype(F32)
    scales = []
    for c in range(per_chunk):
        row = tail[c : c + 1, :] + tail[per_chunk + c : per_chunk + c + 1, :]
        row = lax.rsqrt(row / (heads * BLK) + 1e-06)
        scales.append(jnp.transpose(jnp.broadcast_to(row, (BLK, BLK)))[:, 0:1])
    scale = jnp.concatenate(scales, axis=0)
    mixed = jnp.concatenate([all_ref[h] for h in range(heads)], axis=1)
    stores = []
    for p in range(pieces):
        at = slice(p * wide, (p + 1) * wide)
        out_ref[p] = (dot(mixed, w_ref[:, at]) * scale).astype(BF16)
        stores.append(pltpu.make_async_copy(out_ref.at[p], out_hbm.at[:, at], sems.at[p]))
        stores[p].start()
    for store in stores:
        store.wait()


def project(place, chunks, weight):
    heads = len(chunks)
    rows = chunks[0].shape[0]
    tokens = rows - 16
    width = weight.shape[1]
    pieces = 4
    vmem = pl.BlockSpec(memory_space=pltpu.VMEM)
    body = lambda *refs: project_body(heads, *refs)
    return pl.pallas_call(
        body,
        in_specs=[pl.BlockSpec(memory_space=pltpu.SMEM)] + [vmem] * (heads + 1),
        out_specs=pl.BlockSpec(memory_space=pltpu.HBM),
        out_shape=jax.ShapeDtypeStruct((tokens, width), BF16),
        scratch_shapes=[
            pltpu.VMEM((heads, tokens, BLK), BF16),
            pltpu.VMEM((pieces, tokens, width // pieces), BF16),
            pltpu.SemaphoreType.DMA((pieces,)),
        ],
        compiler_params=params(16),
        cost_estimate=cost(2 * tokens * weight.size, 2 * weight.size),
        name="project",
    )(place, *chunks, weight)


def exchange(x, axes):
    return lax.all_to_all(x, axes, split_axis=0, concat_axis=0, tiled=True)


def from_earlier(shards, axis):
    count = lax.axis_size(axis)
    return [
        lax.ppermute(shard, axis, [(p, (p + k) % count) for p in range(count)])
        for k, shard in enumerate(shards, 1)
    ]


def on_one(
    queries,
    head_key_rows,
    head_value_rows,
    log_input_gate,
    forget_logits,
    head_forget_bias,
    extra_log_forget,
    output_gate_logits,
    head_norm_gain,
    mixer_output_weight,
    second_batch_input,
    expert_norm_gain,
    routed_expert_index,
    routed_copy_weight,
    routed_gate_weight,
    routed_up_weight,
    routed_down_weight,
    shared_gate_weight,
    shared_up_weight,
    shared_down_weight,
):
    length = queries.shape[0]
    ep_count, tp_count = lax.axis_size(EP), lax.axis_size("tp")
    experts = ep_count * tp_count
    cap = 4
    send, normed, slots = dispatch_rows(
        second_batch_input, expert_norm_gain[None, :], routed_expert_index.T, cap, experts
    )
    landed = exchange(send.reshape(experts, 2 * cap, -1), EP_TP)

    def by_block(a):
        return a.reshape(length // BLK, BLK)

    in_gate, forget, extra = (
        by_block(log_input_gate),
        by_block(forget_logits),
        by_block(extra_log_forget),
    )
    query_rows, key_rows = queries.T, head_key_rows.T
    place = jnp.stack([lax.axis_index(a).astype(jnp.int32) for a in ("ep_0", "ep_1", "tp")])
    own = device_state(key_rows, head_value_rows, in_gate, forget, extra, head_forget_bias)
    row_states = [own] + from_earlier([own] * (lax.axis_size("ep_1") - 1), "ep_1")
    row_total = row_state(place, row_states)
    column_states = from_earlier([row_total] * (lax.axis_size("ep_0") - 1), "ep_0")
    chunks = mixer_rows(
        place,
        head_forget_bias,
        row_states,
        column_states,
        query_rows,
        key_rows,
        head_value_rows,
        in_gate,
        forget,
        extra,
        output_gate_logits,
        head_norm_gain[None, :],
        tp_count,
    )
    shared = shared_expert(normed, shared_gate_weight, shared_up_weight, shared_down_weight)
    gathered = [chunks[0]] + from_earlier(chunks[1:], "tp")
    produced = expert_products(landed, routed_gate_weight, routed_up_weight, routed_down_weight)
    back = exchange(produced, EP_TP)
    moe_out, near_weight = combine(
        back.reshape(experts * 2 * cap, -1),
        slots,
        routed_copy_weight.T,
        shared,
        cap,
        mixer_output_weight,
    )
    mixer_first_output = project(place, gathered, near_weight)
    return (mixer_first_output, moe_out)


def solution(mesh):
    split = Mesh(mesh.devices.reshape(4, 4, mesh.shape["tp"]), ("ep_0", "ep_1", "tp"))
    return jax.shard_map(
        on_one,
        mesh=split,
        in_specs=(
            P(EP, "tp"),
            P(EP, "tp"),
            P(EP, "tp"),
            P(EP, "tp"),
            P(EP, "tp"),
            P("tp"),
            P(EP, "tp"),
            P(EP, "tp"),
            P("tp"),
            P(),
            P(EP_TP, None),
            P(),
            P(EP_TP, None),
            P(EP_TP, None),
            P(EP_TP, None, None),
            P(EP_TP, None, None),
            P(EP_TP, None, None),
            P(),
            P(),
            P(),
        ),
        out_specs=(P(EP_TP, None), P(EP_TP, None)),
        check_vma=False,
    )
```

```python
import jax
import jax.numpy as jnp
from jax import lax
from jax.experimental import pallas as pl
from jax.experimental.pallas import tpu as pltpu
from jax.sharding import Mesh
from jax.sharding import PartitionSpec as P


EP = ("ep_0", "ep_1")
EP_TP = ("ep_0", "ep_1", "tp")
BLK = 128
F32 = jnp.float32
BF16 = jnp.bfloat16
NEG = -1e30


def split_two(x):
    hi = x.astype(BF16)
    return hi, (x - hi.astype(F32)).astype(BF16)


def dot(a, b, dims=(((1,), (0,)), ((), ()))):
    return lax.dot_general(a, b, dims, preferred_element_type=F32)


def exact_dot(a, b, dims=(((1,), (0,)), ((), ()))):
    return lax.dot_general(
        a, b, dims, precision=lax.Precision.HIGHEST, preferred_element_type=F32
    )


def iota(shape, dim):
    return lax.broadcasted_iota(jnp.int32, shape, dim)


def params(mib, grid=False):
    return pltpu.CompilerParams(
        vmem_limit_bytes=mib * 2**20,
        dimension_semantics=("arbitrary",) if grid else None,
    )


def in_hbm(*arrays):
    return [pltpu.with_memory_space_constraint(a, pltpu.HBM) for a in arrays]


def cost(flops, nbytes):
    return pl.CostEstimate(flops=int(flops), bytes_accessed=int(nbytes), transcendentals=0)


def copy_slots(idx, cap, experts):
    tokens = idx.shape[1]
    sub = iota((experts, tokens), 0)
    first = sub == idx[0:1, :]
    second = sub == idx[1:2, :]
    named = jnp.where(first | second, 1.0, 0.0).astype(BF16)
    before = jnp.where(iota((tokens, tokens), 0) < iota((tokens, tokens), 1), 1.0, 0.0)
    prior = dot(named, before.astype(BF16))
    places = [jnp.sum(jnp.where(hot, prior, 0.0), axis=0, keepdims=True) for hot in (first, second)]
    return [idx[j : j + 1, :] * cap + places[j].astype(jnp.int32) for j in range(2)]


def start_body(cap, *refs):
    bias_ref = refs[0]
    sources = refs[1:9]
    send_hbm, normed_hbm, slots_hbm, state_ref = refs[9:13]
    (idx_ref, gain_ref, in_ref, forget_ref, extra_ref, k_ref, v_ref, x_ref,
     send_ref, normed_ref, slots_ref, in_sems, out_sems) = refs[13:]
    tokens, width = x_ref.shape
    half = width // 2
    pieces, pairs = send_ref.shape[0:2]
    experts = 2 * pieces * pairs
    kept = (idx_ref, gain_ref, in_ref, forget_ref, extra_ref, k_ref, v_ref, x_ref)
    loads = [
        pltpu.make_async_copy(src, dst, in_sems.at[i])
        for i, (src, dst) in enumerate(zip(sources, kept))
    ]
    for load in loads:
        load.start()
    for load in loads[:-1]:
        load.wait()
    slot0, slot1 = copy_slots(idx_ref[...], cap, experts)
    slots_ref[...] = jnp.concatenate([slot0, slot1] * 4, axis=0)
    stores = [pltpu.make_async_copy(slots_ref, slots_hbm, out_sems.at[pieces])]
    stores[0].start()
    write_state(k_ref, v_ref, in_ref, forget_ref, extra_ref, bias_ref, state_ref)
    loads[-1].wait()
    x = x_ref[...].astype(F32)
    scale = lax.rsqrt(jnp.mean(x * x, axis=-1, keepdims=True) + 1e-06)
    normed = (x * scale * gain_ref[...]).astype(BF16)
    normed_ref[...] = normed
    stores.append(pltpu.make_async_copy(normed_ref, normed_hbm, out_sems.at[pieces + 1]))
    lower = iota((pairs, 8, half), 1) < 4
    rows = pairs * 2 * cap
    for p in range(pieces):
        row = iota((rows, tokens), 0) + p * rows
        wanted = jnp.where((row == slot0) | (row == slot1), 1.0, 0.0).astype(BF16)
        first = dot(wanted, normed_ref[:, :half]).reshape(pairs, 8, half)
        last = dot(wanted, normed_ref[:, half:]).reshape(pairs, 8, half)
        even, odd = swap_halves(first, last, lower)
        send_ref[p, :, 0] = even.astype(BF16)
        send_ref[p, :, 1] = odd.astype(BF16)
        stores.append(pltpu.make_async_copy(send_ref.at[p], send_hbm.at[p], out_sems.at[p]))
        stores[-1].start()
        if p == 0:
            stores[1].start()
    for store in stores:
        store.wait()


def start(x, gain, idx, keys, values, in_gate, forget, extra, bias, cap, experts):
    tokens, width = x.shape
    pieces = 4
    shape = (pieces, experts // (2 * pieces), 2, 2 * cap, width // 2)
    inputs = (idx, gain, in_gate, forget, extra, keys, values, x)
    hbm = pl.BlockSpec(memory_space=pltpu.HBM)
    body = lambda *refs: start_body(cap, *refs)
    return pl.pallas_call(
        body,
        in_specs=[pl.BlockSpec(memory_space=pltpu.SMEM)] + [hbm] * len(inputs),
        out_specs=[hbm] * 3 + [pl.BlockSpec(memory_space=pltpu.VMEM)],
        out_shape=[
            pltpu.HBM(shape, BF16),
            pltpu.HBM((tokens, width), BF16),
            pltpu.HBM((8, tokens), jnp.int32),
            jax.ShapeDtypeStruct((keys.shape[0] + 8, BLK), F32),
        ],
        scratch_shapes=[pltpu.VMEM(a.shape, a.dtype) for a in inputs]
        + [
            pltpu.VMEM(shape, BF16),
            pltpu.VMEM((tokens, width), BF16),
            pltpu.VMEM((8, tokens), jnp.int32),
            pltpu.SemaphoreType.DMA((len(inputs),)),
            pltpu.SemaphoreType.DMA((pieces + 2,)),
        ],
        compiler_params=params(24),
        cost_estimate=cost(2 * experts * cap * tokens * width, 4 * experts * cap * width),
        name="start",
    )(bias, *in_hbm(*inputs))


def swap_halves(even, odd, lower):
    first = jnp.where(lower, even, pltpu.roll(odd, 4, 1))
    last = jnp.where(lower, pltpu.roll(even, 4, 1), odd)
    return first, last


def expert_body(pieces, a_ref, g_hbm, u_hbm, d_hbm, out_hbm, x_ref, h_ref, g_ref, u_ref, d_ref, o_ref, sems):
    pairs = a_ref.shape[0]
    half = a_ref.shape[3]
    hidden = h_ref.shape[1]
    group = 8
    wide = hidden // pieces
    part = half // pieces
    first_loads, last_loads, stores = [], [], []
    for p in range(pieces):
        at = slice(p * wide, (p + 1) * wide)
        first_loads.append(
            [
                pltpu.make_async_copy(g_hbm.at[0, :, at], g_ref.at[p], sems.at[0, p]),
                pltpu.make_async_copy(u_hbm.at[0, :, at], u_ref.at[p], sems.at[1, p]),
            ]
        )
        at = slice(p * part, (p + 1) * part)
        other = slice(half + p * part, half + (p + 1) * part)
        last_loads.append(
            [
                pltpu.make_async_copy(d_hbm.at[0, :, at], d_ref.at[p, 0], sems.at[2, p]),
                pltpu.make_async_copy(d_hbm.at[0, :, other], d_ref.at[p, 1], sems.at[3, p]),
            ]
        )
        stores.append(pltpu.make_async_copy(o_ref.at[p], out_hbm.at[:, :, :, at], sems.at[4, p]))
    for copies in first_loads + last_loads:
        for copy in copies:
            copy.start()
    lower = iota((group, 8, half), 1) < 4
    for i in range(pairs // group):
        tiles = a_ref[i * group : (i + 1) * group].astype(F32)
        first, last = swap_halves(tiles[:, 0], tiles[:, 1], lower)
        at = slice(i * group * 8, (i + 1) * group * 8)
        x_ref[at, 0:half] = first.reshape(group * 8, half).astype(BF16)
        x_ref[at, half:] = last.reshape(group * 8, half).astype(BF16)

    lower = iota((pairs, 8, part), 1) < 4

    def activate(p, gate, up):
        h_ref[:, p * wide : (p + 1) * wide] = (gate * jax.nn.sigmoid(gate) * up).astype(BF16)

    def leave(p, first, last):
        even, odd = swap_halves(first.reshape(pairs, 8, part), last.reshape(pairs, 8, part), lower)
        o_ref[p, :, 0] = even.astype(BF16)
        o_ref[p, :, 1] = odd.astype(BF16)
        stores[p].start()

    ahead = None
    for p in range(pieces):
        for copy in first_loads[p]:
            copy.wait()
        x = x_ref[...]
        products = (dot(x, g_ref[p]), dot(x, u_ref[p]))
        if ahead is not None:
            activate(p - 1, *ahead)
        ahead = products
    activate(pieces - 1, *ahead)
    ahead = None
    for copies in last_loads:
        for copy in copies:
            copy.wait()
    for p in range(pieces):
        h = h_ref[...]
        products = (dot(h, d_ref[p, 0]), dot(h, d_ref[p, 1]))
        if ahead is not None:
            leave(p - 1, *ahead)
        ahead = products
    leave(pieces - 1, *ahead)
    for store in stores:
        store.wait()


def expert_products(arrived, gate_weight, up_weight, down_weight):
    count, rows, half = arrived.shape
    _, width, hidden = gate_weight.shape
    pieces = 4
    shape = (count // 2, 2, rows, half)
    slots = count * rows // 2
    hbm = pl.BlockSpec(memory_space=pltpu.HBM)
    body = lambda *refs: expert_body(pieces, *refs)
    out = pl.pallas_call(
        body,
        in_specs=[pl.BlockSpec(memory_space=pltpu.VMEM), hbm, hbm, hbm],
        out_specs=hbm,
        out_shape=pltpu.HBM(shape, BF16),
        scratch_shapes=[
            pltpu.VMEM((slots, width), BF16),
            pltpu.VMEM((slots, hidden), BF16),
            pltpu.VMEM((pieces, width, hidden // pieces), BF16),
            pltpu.VMEM((pieces, width, hidden // pieces), BF16),
            pltpu.VMEM((pieces, 2, hidden, half // pieces), BF16),
            pltpu.VMEM((pieces, count // 2, 2, rows, half // pieces), BF16),
            pltpu.SemaphoreType.DMA((5, pieces)),
        ],
        compiler_params=params(32),
        cost_estimate=cost(3 * count * rows * width * hidden, 6 * width * hidden),
        name="expert_products",
    )(arrived.reshape(shape), *in_hbm(gate_weight, up_weight, down_weight))
    return out.reshape(arrived.shape)


def shared_body(n_ref, g_ref, u_ref, d_ref, out_ref):
    normed = n_ref[...]
    gate = dot(normed, g_ref[...])
    up = dot(normed, u_ref[...])
    hidden = (gate * jax.nn.sigmoid(gate) * up).astype(BF16)
    out_ref[...] = dot(hidden, d_ref[...])


def shared_expert(normed, gate_weight, up_weight, down_weight):
    tokens, width = normed.shape
    hidden = gate_weight.shape[1]
    return pl.pallas_call(
        shared_body,
        out_shape=pltpu.HBM((tokens, width), F32),
        compiler_params=params(16),
        cost_estimate=cost(6 * tokens * width * hidden, 6 * width * hidden),
        name="shared_expert",
    )(*in_hbm(normed, gate_weight, up_weight, down_weight))


def combine_body(
    cap, back_ref, slots_ref, weight_ref, shared_hbm, w_hbm, out_hbm, w_ref, shared_ref, out_ref, sems, w_sem
):
    tokens, _ = out_ref.shape
    total, half = back_ref.shape
    loads, stores = [], []
    for h in range(2):
        cols = slice(h * half, (h + 1) * half)
        loads.append(
            pltpu.make_async_copy(shared_hbm.at[:, cols], shared_ref.at[:, cols], sems.at[0, h])
        )
        stores.append(pltpu.make_async_copy(out_ref.at[:, cols], out_hbm.at[:, cols], sems.at[1, h]))
        loads[h].start()
    bring = pltpu.make_async_copy(w_hbm, w_ref, w_sem)
    bring.start()
    slot_col = jnp.transpose(slots_ref[...].astype(F32)).astype(jnp.int32)
    weight_col = jnp.transpose(jnp.concatenate([weight_ref[...]] * 4, axis=0)).astype(BF16)
    lane = iota((tokens, total), 1)
    at = [(s // cap) * (2 * cap) + s % cap for s in (slot_col[:, 0:1], slot_col[:, 1:2])]
    for h in range(2):
        cols = slice(h * half, (h + 1) * half)
        mix = jnp.where(
            lane == at[0] + h * cap,
            weight_col[:, 0:1].astype(F32),
            jnp.where(lane == at[1] + h * cap, weight_col[:, 1:2].astype(F32), 0.0),
        ).astype(BF16)
        routed = dot(mix, back_ref[...])
        loads[h].wait()
        out_ref[:, cols] = (routed + shared_ref[:, cols]).astype(BF16)
        stores[h].start()
    for store in stores:
        store.wait()
    bring.wait()


def combine(back, slots, weights, shared, cap, mixer_weight):
    tokens, width = shared.shape
    hbm = pl.BlockSpec(memory_space=pltpu.HBM)
    vmem = pl.BlockSpec(memory_space=pltpu.VMEM)
    body = lambda *refs: combine_body(cap, *refs)
    return pl.pallas_call(
        body,
        in_specs=[vmem, vmem, vmem, hbm, hbm],
        out_specs=[hbm, vmem],
        out_shape=[
            jax.ShapeDtypeStruct((tokens, width), BF16),
            pltpu.VMEM(mixer_weight.shape, BF16),
        ],
        scratch_shapes=[
            pltpu.VMEM((tokens, width), F32),
            pltpu.VMEM((tokens, width), BF16),
            pltpu.SemaphoreType.DMA((2, 2)),
            pltpu.SemaphoreType.DMA,
        ],
        compiler_params=params(20),
        cost_estimate=cost(4 * tokens * back.shape[0] * width, 2 * back.size),
        name="combine",
    )(back, slots, weights, *in_hbm(shared, mixer_weight))


def gate_rows(in_ref, forget_ref, extra_ref, bias):
    x = forget_ref[...] + bias
    log_forget = jnp.minimum(x, 0.0) - jnp.log1p(jnp.exp(-jnp.abs(x))) + extra_ref[...]
    upper = jnp.where(iota((BLK, BLK), 0) <= iota((BLK, BLK), 1), 1.0, 0.0)
    cumulative = exact_dot(log_forget, upper)
    ones = jnp.ones((BLK, BLK), F32)
    total = exact_dot(log_forget, ones)
    return in_ref[...], cumulative, total


def write_state(k_ref, v_ref, in_ref, forget_ref, extra_ref, bias_ref, out_ref):
    key_dim, length = k_ref.shape
    blocks = length // BLK
    in_gate, cumulative, total = gate_rows(in_ref, forget_ref, extra_ref, bias_ref[0])
    sums = [jnp.zeros((1, BLK), F32)]
    for j in reversed(range(1, blocks)):
        sums.insert(0, sums[0] + total[j : j + 1, :])
    after = jnp.concatenate(sums, axis=0)
    gap = after + total - cumulative + in_gate
    top = jnp.max(jnp.max(gap, axis=1, keepdims=True), axis=0, keepdims=True)
    weight = jnp.exp(gap - top)
    decay = jnp.sum(total[:, 0:1], axis=0, keepdims=True)
    acc = jnp.zeros((2 * key_dim, 2 * BLK), F32)
    ones = jnp.ones((2 * BLK, BLK), BF16)
    for j in range(blocks // 2):
        at = slice(j * 2 * BLK, (j + 1) * 2 * BLK)
        weights = jnp.concatenate([weight[2 * j : 2 * j + 1], weight[2 * j + 1 : 2 * j + 2]], axis=1)
        keys = k_ref[:, at].astype(F32) * weights
        hi, lo = split_two(keys)
        values = jnp.concatenate([v_ref[at, :], ones], axis=1)
        acc = acc + dot(jnp.concatenate([hi, lo], axis=0), values)
    state = acc[:key_dim] + acc[key_dim:]
    norm = jnp.transpose(state[:, BLK:])[0:8, :]
    norm = jnp.concatenate([norm, jnp.zeros((8, BLK - key_dim), F32)], axis=1)
    lane = iota((8, BLK), 1)
    tail = jnp.where(lane < key_dim, norm, jnp.where(lane < key_dim + 32, top, decay))
    out_ref[0:key_dim, :] = state[:, 0:BLK]
    out_ref[key_dim:, :] = tail


def merge_states(refs, keys, counted, key_dim):
    tails = [ref[key_dim : key_dim + 1, :] for ref in refs]
    tops = [t[:, key_dim : key_dim + 1] for t in tails]
    decays = [
        jnp.where(c, t[:, key_dim + 32 : key_dim + 33], 0.0) for t, c in zip(tails, counted)
    ]
    gaps = []
    for i, key in enumerate(keys):
        since = jnp.zeros((1, 1), F32)
        for j, other in enumerate(keys):
            if j != i:
                since = since + jnp.where(other > key, decays[j], 0.0)
        gaps.append(jnp.where(counted[i], tops[i] + since, NEG))
    top = gaps[0]
    for gap in gaps[1:]:
        top = jnp.maximum(top, gap)
    merged = jnp.zeros((key_dim + 8, BLK), F32)
    for ref, gap, c in zip(refs, gaps, counted):
        merged = merged + ref[...] * jnp.where(c, jnp.exp(gap - top), 0.0)
    return merged, top, sum(decays)


def as_one(scalar):
    return jnp.full((1, 1), scalar, jnp.int32)


def ring_places(place, count):
    return [as_one((place + count - k) % count) for k in range(count)]


def row_body(place_ref, *refs):
    *states, out_ref = refs
    key_dim = out_ref.shape[0] - 8
    keys = ring_places(place_ref[1], len(states))
    counted = [jnp.full((1, 1), True)] * len(states)
    merged, top, decay = merge_states(states, keys, counted, key_dim)
    lane = iota((8, BLK), 1)
    norm = merged[key_dim:, :]
    out_ref[0:key_dim, :] = merged[0:key_dim]
    out_ref[key_dim:, :] = jnp.where(
        lane < key_dim, norm, jnp.where(lane < key_dim + 32, top, decay)
    )


def row_state(place, states):
    return pl.pallas_call(
        row_body,
        in_specs=[pl.BlockSpec(memory_space=pltpu.SMEM)]
        + [pl.BlockSpec(memory_space=pltpu.VMEM)] * len(states),
        out_shape=jax.ShapeDtypeStruct(states[0].shape, F32),
        compiler_params=params(4),
        cost_estimate=cost(2**20, 2**18),
        name="row_state",
    )(place, *states)


def incoming_state(place_ref, rows, columns, key_dim):
    in_row = ring_places(place_ref[1], len(rows))
    in_column = ring_places(place_ref[0], len(columns) + 1)[1:]
    counted = [p < as_one(place_ref[1]) for p in in_row[1:]]
    counted += [p < as_one(place_ref[0]) for p in in_column]
    keys = [p + len(columns) + 1 for p in in_row[1:]] + in_column
    memory, top, _ = merge_states(rows[1:] + columns, keys, counted, key_dim)
    norm = jnp.broadcast_to(memory[key_dim : key_dim + 1, :], (BLK, BLK))
    norm = jnp.transpose(norm)[0:key_dim, :]
    return jnp.concatenate([memory[0:key_dim], norm], axis=1), top


def mixer_body(
    rows_count,
    columns_count,
    place_ref,
    bias_ref,
    q_ref,
    k_ref,
    v_ref,
    in_ref,
    forget_ref,
    extra_ref,
    gate_ref,
    gain_ref,
    *refs,
):
    key_dim, length = k_ref.shape
    blocks = length // BLK
    rows = list(refs[:rows_count])
    columns = list(refs[rows_count : rows_count + columns_count])
    *outs, out_ref = refs[rows_count + columns_count :]
    peers = len(outs)
    tokens = length // peers
    per_chunk = tokens // BLK
    in_gate, cumulative, total = gate_rows(in_ref, forget_ref, extra_ref, bias_ref[0])
    state, top = incoming_state(place_ref, rows, columns, key_dim)
    gap = total - cumulative + in_gate
    block_top = jnp.max(gap, axis=1, keepdims=True)
    weight = jnp.exp(gap - block_top)
    shifted = in_gate - cumulative
    sum_col = jnp.transpose(jnp.concatenate([cumulative] * (BLK // blocks), axis=0))
    ones = jnp.ones((BLK, BLK), BF16)
    lower = iota((BLK, BLK), 1) <= iota((BLK, BLK), 0)
    gain = gain_ref[...]
    eight = jnp.ones((8, BLK), F32)
    squares = []
    for j in range(blocks):
        at = slice(j * BLK, (j + 1) * BLK)
        keys = k_ref[:, at]
        values = jnp.concatenate([v_ref[at, :], ones], axis=1)
        query = jnp.transpose(q_ref[:, at].astype(F32) * (key_dim**-0.5)).astype(BF16)
        base = sum_col[:, j : j + 1]
        pair = jnp.where(lower, base + shifted[j : j + 1, :], -jnp.inf)
        carried = base + top
        stable = jnp.maximum(carried, jnp.max(pair, axis=1, keepdims=True))
        scores = dot(query, keys) * jnp.exp(pair - stable)
        carry = jnp.exp(carried - stable)
        score_hi, score_lo = split_two(scores)
        state_hi, state_lo = split_two(state)
        both = dot(score_hi, values) + dot(score_lo, values)
        both = both + carry * (dot(query, state_hi) + dot(query, state_lo))
        hidden = both[:, :BLK] / jnp.maximum(jnp.abs(both[:, BLK:]), jnp.exp(-stable))
        squares.append(
            exact_dot(eight, hidden * hidden, (((1,), (1,)), ((), ())))[0:1, :]
        )
        gated = hidden * gain * jax.nn.sigmoid(gate_ref[at, :].astype(F32))
        start = (j % per_chunk) * BLK
        out_ref[j // per_chunk, start : start + BLK, :] = gated.astype(BF16)
        if j + 1 < blocks:
            hi, lo = split_two(keys.astype(F32) * weight[j : j + 1, :])
            added = dot(jnp.concatenate([hi, lo], axis=0), values)
            added = added[:key_dim] + added[key_dim:]
            late = block_top[j : j + 1, :]
            early = total[j : j + 1, 0:1] + top
            top = jnp.maximum(early, late)
            state = jnp.exp(early - top) * state + jnp.exp(late - top) * added
    for c in range(peers):
        own = squares[c * per_chunk : (c + 1) * per_chunk]
        parts = [split_two(row) for row in own]
        rows = [hi.astype(F32) for hi, _ in parts] + [lo.astype(F32) for _, lo in parts]
        rows.append(jnp.zeros((16 - len(rows), BLK), F32))
        out_ref[c, tokens:, :] = jnp.concatenate(rows, axis=0).astype(BF16)
    for k in range(peers):
        outs[k][...] = out_ref[(place_ref[2] + k) % peers]


def mixer_rows(place, bias, rows, columns, queries, keys, values, in_gate, forget, extra, gate, gain, peers):
    _, length = keys.shape
    smem = pl.BlockSpec(memory_space=pltpu.SMEM)
    vmem = pl.BlockSpec(memory_space=pltpu.VMEM)
    chunk = (length // peers + 16, BLK)
    body = lambda *refs: mixer_body(len(rows), len(columns), *refs)
    return pl.pallas_call(
        body,
        in_specs=[smem, smem] + [vmem] * (8 + len(rows) + len(columns)),
        out_shape=[jax.ShapeDtypeStruct(chunk, BF16)] * peers,
        scratch_shapes=[pltpu.VMEM((peers, *chunk), BF16)],
        compiler_params=params(16),
        cost_estimate=cost(32 * length * BLK * BLK, 8 * length * BLK),
        name="mixer_rows",
    )(
        place,
        bias,
        *in_hbm(queries, keys, values, in_gate, forget, extra, gate, gain),
        *rows,
        *columns,
    )


def project_body(heads, place_ref, *refs):
    chunks = refs[:heads]
    w_ref, out_hbm, all_ref, out_ref, sems = refs[heads:]
    pieces, tokens, wide = out_ref.shape
    per_chunk = tokens // BLK
    for k in range(heads):
        all_ref[(place_ref[2] + heads - k) % heads] = chunks[k][0:tokens, :]
    tail = chunks[0][tokens:, :].astype(F32)
    for k in range(1, heads):
        tail = tail + chunks[k][tokens:, :].astype(F32)
    scales = []
    for c in range(per_chunk):
        row = tail[c : c + 1, :] + tail[per_chunk + c : per_chunk + c + 1, :]
        row = lax.rsqrt(row / (heads * BLK) + 1e-06)
        scales.append(jnp.transpose(jnp.broadcast_to(row, (BLK, BLK)))[:, 0:1])
    scale = jnp.concatenate(scales, axis=0)
    mixed = jnp.concatenate([all_ref[h] for h in range(heads)], axis=1)
    stores = []
    for p in range(pieces):
        at = slice(p * wide, (p + 1) * wide)
        out_ref[p] = (dot(mixed, w_ref[:, at]) * scale).astype(BF16)
        stores.append(pltpu.make_async_copy(out_ref.at[p], out_hbm.at[:, at], sems.at[p]))
        stores[p].start()
    for store in stores:
        store.wait()


def project(place, chunks, weight):
    heads = len(chunks)
    rows = chunks[0].shape[0]
    tokens = rows - 16
    width = weight.shape[1]
    pieces = 4
    vmem = pl.BlockSpec(memory_space=pltpu.VMEM)
    body = lambda *refs: project_body(heads, *refs)
    return pl.pallas_call(
        body,
        in_specs=[pl.BlockSpec(memory_space=pltpu.SMEM)] + [vmem] * (heads + 1),
        out_specs=pl.BlockSpec(memory_space=pltpu.HBM),
        out_shape=jax.ShapeDtypeStruct((tokens, width), BF16),
        scratch_shapes=[
            pltpu.VMEM((heads, tokens, BLK), BF16),
            pltpu.VMEM((pieces, tokens, width // pieces), BF16),
            pltpu.SemaphoreType.DMA((pieces,)),
        ],
        compiler_params=params(16),
        cost_estimate=cost(2 * tokens * weight.size, 2 * weight.size),
        name="project",
    )(place, *chunks, weight)


def exchange(x, axes):
    return lax.all_to_all(x, axes, split_axis=0, concat_axis=0, tiled=True)


def from_earlier(shards, axis):
    count = lax.axis_size(axis)
    return [
        lax.ppermute(shard, axis, [(p, (p + k) % count) for p in range(count)])
        for k, shard in enumerate(shards, 1)
    ]


def on_one(
    queries,
    head_key_rows,
    head_value_rows,
    log_input_gate,
    forget_logits,
    head_forget_bias,
    extra_log_forget,
    output_gate_logits,
    head_norm_gain,
    mixer_output_weight,
    second_batch_input,
    expert_norm_gain,
    routed_expert_index,
    routed_copy_weight,
    routed_gate_weight,
    routed_up_weight,
    routed_down_weight,
    shared_gate_weight,
    shared_up_weight,
    shared_down_weight,
):
    length = queries.shape[0]
    ep_count, tp_count = lax.axis_size(EP), lax.axis_size("tp")
    experts = ep_count * tp_count
    cap = 4

    def by_block(a):
        return a.reshape(length // BLK, BLK)

    in_gate, forget, extra = (
        by_block(log_input_gate),
        by_block(forget_logits),
        by_block(extra_log_forget),
    )
    query_rows, key_rows = queries.T, head_key_rows.T
    send, normed, slots, own = start(
        second_batch_input,
        expert_norm_gain[None, :],
        routed_expert_index.T,
        key_rows,
        head_value_rows,
        in_gate,
        forget,
        extra,
        head_forget_bias,
        cap,
        experts,
    )
    place = jnp.stack([lax.axis_index(a).astype(jnp.int32) for a in ("ep_0", "ep_1", "tp")])
    row_states = [own] + from_earlier([own] * (lax.axis_size("ep_1") - 1), "ep_1")
    row_total = row_state(place, row_states)
    column_states = from_earlier([row_total] * (lax.axis_size("ep_0") - 1), "ep_0")
    landed = exchange(send.reshape(experts, 2 * cap, -1), EP_TP)
    chunks = mixer_rows(
        place,
        head_forget_bias,
        row_states,
        column_states,
        query_rows,
        key_rows,
        head_value_rows,
        in_gate,
        forget,
        extra,
        output_gate_logits,
        head_norm_gain[None, :],
        tp_count,
    )
    shared = shared_expert(normed, shared_gate_weight, shared_up_weight, shared_down_weight)
    gathered = [chunks[0]] + from_earlier(chunks[1:], "tp")
    produced = expert_products(landed, routed_gate_weight, routed_up_weight, routed_down_weight)
    back = exchange(produced, EP_TP)
    moe_out, near_weight = combine(
        back.reshape(experts * 2 * cap, -1),
        slots,
        routed_copy_weight.T,
        shared,
        cap,
        mixer_output_weight,
    )
    mixer_first_output = project(place, gathered, near_weight)
    return (mixer_first_output, moe_out)


def solution(mesh):
    split = Mesh(mesh.devices.reshape(4, 4, mesh.shape["tp"]), ("ep_0", "ep_1", "tp"))
    return jax.shard_map(
        on_one,
        mesh=split,
        in_specs=(
            P(EP, "tp"),
            P(EP, "tp"),
            P(EP, "tp"),
            P(EP, "tp"),
            P(EP, "tp"),
            P("tp"),
            P(EP, "tp"),
            P(EP, "tp"),
            P("tp"),
            P(),
            P(EP_TP, None),
            P(),
            P(EP_TP, None),
            P(EP_TP, None),
            P(EP_TP, None, None),
            P(EP_TP, None, None),
            P(EP_TP, None, None),
            P(),
            P(),
            P(),
        ),
        out_specs=(P(EP_TP, None), P(EP_TP, None)),
        check_vma=False,
    )
```

```python
import jax
import jax.numpy as jnp
from jax import lax
from jax.experimental import pallas as pl
from jax.experimental.pallas import tpu as pltpu
from jax.sharding import Mesh
from jax.sharding import PartitionSpec as P


EP = ("ep_0", "ep_1")
EP_TP = ("ep_0", "ep_1", "tp")
BLK = 128
F32 = jnp.float32
BF16 = jnp.bfloat16
NEG = -1e30


def split_two(x):
    hi = x.astype(BF16)
    return hi, (x - hi.astype(F32)).astype(BF16)


def dot(a, b, dims=(((1,), (0,)), ((), ()))):
    return lax.dot_general(a, b, dims, preferred_element_type=F32)


def exact_dot(a, b, dims=(((1,), (0,)), ((), ()))):
    return lax.dot_general(
        a, b, dims, precision=lax.Precision.HIGHEST, preferred_element_type=F32
    )


def iota(shape, dim):
    return lax.broadcasted_iota(jnp.int32, shape, dim)


def params(mib, grid=False):
    return pltpu.CompilerParams(
        vmem_limit_bytes=mib * 2**20,
        dimension_semantics=("arbitrary",) if grid else None,
    )


def in_hbm(*arrays):
    return [pltpu.with_memory_space_constraint(a, pltpu.HBM) for a in arrays]


def cost(flops, nbytes):
    return pl.CostEstimate(flops=int(flops), bytes_accessed=int(nbytes), transcendentals=0)


def copy_slots(idx, cap, experts):
    tokens = idx.shape[1]
    sub = iota((experts, tokens), 0)
    first = sub == idx[0:1, :]
    second = sub == idx[1:2, :]
    named = jnp.where(first | second, 1.0, 0.0).astype(BF16)
    before = jnp.where(iota((tokens, tokens), 0) < iota((tokens, tokens), 1), 1.0, 0.0)
    prior = dot(named, before.astype(BF16))
    places = [jnp.sum(jnp.where(hot, prior, 0.0), axis=0, keepdims=True) for hot in (first, second)]
    return [idx[j : j + 1, :] * cap + places[j].astype(jnp.int32) for j in range(2)]


def start_body(cap, *refs):
    bias_ref = refs[0]
    sources = refs[1:9]
    send_hbm, normed_hbm, slots_hbm, state_ref = refs[9:13]
    (idx_ref, gain_ref, in_ref, forget_ref, extra_ref, k_ref, v_ref, x_ref,
     send_ref, normed_ref, slots_ref, in_sems, out_sems) = refs[13:]
    tokens, width = x_ref.shape
    half = width // 2
    pieces, pairs = send_ref.shape[0:2]
    experts = 2 * pieces * pairs
    kept = (idx_ref, gain_ref, in_ref, forget_ref, extra_ref, k_ref, v_ref, x_ref)
    loads = [
        pltpu.make_async_copy(src, dst, in_sems.at[i])
        for i, (src, dst) in enumerate(zip(sources, kept))
    ]
    for load in loads:
        load.start()
    for load in loads[:-1]:
        load.wait()
    slot0, slot1 = copy_slots(idx_ref[...], cap, experts)
    slots_ref[...] = jnp.concatenate([slot0, slot1] * 4, axis=0)
    stores = [pltpu.make_async_copy(slots_ref, slots_hbm, out_sems.at[pieces])]
    stores[0].start()
    write_state(k_ref, v_ref, in_ref, forget_ref, extra_ref, bias_ref, state_ref)
    loads[-1].wait()
    x = x_ref[...].astype(F32)
    scale = lax.rsqrt(jnp.mean(x * x, axis=-1, keepdims=True) + 1e-06)
    normed = (x * scale * gain_ref[...]).astype(BF16)
    normed_ref[...] = normed
    stores.append(pltpu.make_async_copy(normed_ref, normed_hbm, out_sems.at[pieces + 1]))
    lower = iota((pairs, 8, half), 1) < 4
    rows = pairs * 2 * cap
    for p in range(pieces):
        row = iota((rows, tokens), 0) + p * rows
        wanted = jnp.where((row == slot0) | (row == slot1), 1.0, 0.0).astype(BF16)
        first = dot(wanted, normed_ref[:, :half]).reshape(pairs, 8, half)
        last = dot(wanted, normed_ref[:, half:]).reshape(pairs, 8, half)
        even, odd = swap_halves(first, last, lower)
        send_ref[p, :, 0] = even.astype(BF16)
        send_ref[p, :, 1] = odd.astype(BF16)
        stores.append(pltpu.make_async_copy(send_ref.at[p], send_hbm.at[p], out_sems.at[p]))
        stores[-1].start()
        if p == 0:
            stores[1].start()
    for store in stores:
        store.wait()


def start(x, gain, idx, keys, values, in_gate, forget, extra, bias, cap, experts):
    tokens, width = x.shape
    pieces = 2
    shape = (pieces, experts // (2 * pieces), 2, 2 * cap, width // 2)
    inputs = (idx, gain, in_gate, forget, extra, keys, values, x)
    hbm = pl.BlockSpec(memory_space=pltpu.HBM)
    body = lambda *refs: start_body(cap, *refs)
    return pl.pallas_call(
        body,
        in_specs=[pl.BlockSpec(memory_space=pltpu.SMEM)] + [hbm] * len(inputs),
        out_specs=[hbm] * 3 + [pl.BlockSpec(memory_space=pltpu.VMEM)],
        out_shape=[
            pltpu.HBM(shape, BF16),
            pltpu.HBM((tokens, width), BF16),
            pltpu.HBM((8, tokens), jnp.int32),
            jax.ShapeDtypeStruct((keys.shape[0] + 8, BLK), F32),
        ],
        scratch_shapes=[pltpu.VMEM(a.shape, a.dtype) for a in inputs]
        + [
            pltpu.VMEM(shape, BF16),
            pltpu.VMEM((tokens, width), BF16),
            pltpu.VMEM((8, tokens), jnp.int32),
            pltpu.SemaphoreType.DMA((len(inputs),)),
            pltpu.SemaphoreType.DMA((pieces + 2,)),
        ],
        compiler_params=params(24),
        cost_estimate=cost(2 * experts * cap * tokens * width, 4 * experts * cap * width),
        name="start",
    )(bias, *in_hbm(*inputs))


def swap_halves(even, odd, lower):
    first = jnp.where(lower, even, pltpu.roll(odd, 4, 1))
    last = jnp.where(lower, pltpu.roll(even, 4, 1), odd)
    return first, last


def expert_body(pieces, a_ref, g_hbm, u_hbm, d_hbm, out_hbm, x_ref, h_ref, g_ref, u_ref, d_ref, o_ref, sems):
    pairs = a_ref.shape[0]
    half = a_ref.shape[3]
    hidden = h_ref.shape[1]
    group = 8
    wide = hidden // pieces
    part = half // pieces
    first_loads, last_loads, stores = [], [], []
    for p in range(pieces):
        at = slice(p * wide, (p + 1) * wide)
        first_loads.append(
            [
                pltpu.make_async_copy(g_hbm.at[0, :, at], g_ref.at[p], sems.at[0, p]),
                pltpu.make_async_copy(u_hbm.at[0, :, at], u_ref.at[p], sems.at[1, p]),
            ]
        )
        at = slice(p * part, (p + 1) * part)
        other = slice(half + p * part, half + (p + 1) * part)
        last_loads.append(
            [
                pltpu.make_async_copy(d_hbm.at[0, :, at], d_ref.at[p, 0], sems.at[2, p]),
                pltpu.make_async_copy(d_hbm.at[0, :, other], d_ref.at[p, 1], sems.at[3, p]),
            ]
        )
        stores.append(pltpu.make_async_copy(o_ref.at[p], out_hbm.at[:, :, :, at], sems.at[4, p]))
    for copies in first_loads + last_loads:
        for copy in copies:
            copy.start()
    lower = iota((group, 8, half), 1) < 4
    for i in range(pairs // group):
        tiles = a_ref[i * group : (i + 1) * group].astype(F32)
        first, last = swap_halves(tiles[:, 0], tiles[:, 1], lower)
        at = slice(i * group * 8, (i + 1) * group * 8)
        x_ref[at, 0:half] = first.reshape(group * 8, half).astype(BF16)
        x_ref[at, half:] = last.reshape(group * 8, half).astype(BF16)

    lower = iota((pairs, 8, part), 1) < 4

    def activate(p, gate, up):
        h_ref[:, p * wide : (p + 1) * wide] = (gate * jax.nn.sigmoid(gate) * up).astype(BF16)

    def leave(p, first, last):
        even, odd = swap_halves(first.reshape(pairs, 8, part), last.reshape(pairs, 8, part), lower)
        o_ref[p, :, 0] = even.astype(BF16)
        o_ref[p, :, 1] = odd.astype(BF16)
        stores[p].start()

    ahead = None
    for p in range(pieces):
        for copy in first_loads[p]:
            copy.wait()
        x = x_ref[...]
        products = (dot(x, g_ref[p]), dot(x, u_ref[p]))
        if ahead is not None:
            activate(p - 1, *ahead)
        ahead = products
    activate(pieces - 1, *ahead)
    ahead = None
    for copies in last_loads:
        for copy in copies:
            copy.wait()
    for p in range(pieces):
        h = h_ref[...]
        products = (dot(h, d_ref[p, 0]), dot(h, d_ref[p, 1]))
        if ahead is not None:
            leave(p - 1, *ahead)
        ahead = products
    leave(pieces - 1, *ahead)
    for store in stores:
        store.wait()


def expert_products(arrived, gate_weight, up_weight, down_weight):
    count, rows, half = arrived.shape
    _, width, hidden = gate_weight.shape
    pieces = 4
    shape = (count // 2, 2, rows, half)
    slots = count * rows // 2
    hbm = pl.BlockSpec(memory_space=pltpu.HBM)
    body = lambda *refs: expert_body(pieces, *refs)
    out = pl.pallas_call(
        body,
        in_specs=[pl.BlockSpec(memory_space=pltpu.VMEM), hbm, hbm, hbm],
        out_specs=hbm,
        out_shape=pltpu.HBM(shape, BF16),
        scratch_shapes=[
            pltpu.VMEM((slots, width), BF16),
            pltpu.VMEM((slots, hidden), BF16),
            pltpu.VMEM((pieces, width, hidden // pieces), BF16),
            pltpu.VMEM((pieces, width, hidden // pieces), BF16),
            pltpu.VMEM((pieces, 2, hidden, half // pieces), BF16),
            pltpu.VMEM((pieces, count // 2, 2, rows, half // pieces), BF16),
            pltpu.SemaphoreType.DMA((5, pieces)),
        ],
        compiler_params=params(32),
        cost_estimate=cost(3 * count * rows * width * hidden, 6 * width * hidden),
        name="expert_products",
    )(arrived.reshape(shape), *in_hbm(gate_weight, up_weight, down_weight))
    return out.reshape(arrived.shape)


def shared_body(n_ref, g_ref, u_ref, d_ref, out_ref):
    normed = n_ref[...]
    gate = dot(normed, g_ref[...])
    up = dot(normed, u_ref[...])
    hidden = (gate * jax.nn.sigmoid(gate) * up).astype(BF16)
    out_ref[...] = dot(hidden, d_ref[...])


def shared_expert(normed, gate_weight, up_weight, down_weight):
    tokens, width = normed.shape
    hidden = gate_weight.shape[1]
    return pl.pallas_call(
        shared_body,
        out_shape=pltpu.HBM((tokens, width), F32),
        compiler_params=params(16),
        cost_estimate=cost(6 * tokens * width * hidden, 6 * width * hidden),
        name="shared_expert",
    )(*in_hbm(normed, gate_weight, up_weight, down_weight))


def combine_body(
    cap, back_ref, slots_ref, weight_ref, shared_hbm, w_hbm, out_hbm, w_ref, shared_ref, out_ref, sems, w_sem
):
    tokens, _ = out_ref.shape
    total, half = back_ref.shape
    loads, stores = [], []
    for h in range(2):
        cols = slice(h * half, (h + 1) * half)
        loads.append(
            pltpu.make_async_copy(shared_hbm.at[:, cols], shared_ref.at[:, cols], sems.at[0, h])
        )
        stores.append(pltpu.make_async_copy(out_ref.at[:, cols], out_hbm.at[:, cols], sems.at[1, h]))
        loads[h].start()
    bring = pltpu.make_async_copy(w_hbm, w_ref, w_sem)
    bring.start()
    slot_col = jnp.transpose(slots_ref[...].astype(F32)).astype(jnp.int32)
    weight_col = jnp.transpose(jnp.concatenate([weight_ref[...]] * 4, axis=0)).astype(BF16)
    lane = iota((tokens, total), 1)
    at = [(s // cap) * (2 * cap) + s % cap for s in (slot_col[:, 0:1], slot_col[:, 1:2])]
    mix = [
        jnp.where(
            lane == at[0] + h * cap,
            weight_col[:, 0:1].astype(F32),
            jnp.where(lane == at[1] + h * cap, weight_col[:, 1:2].astype(F32), 0.0),
        ).astype(BF16)
        for h in range(2)
    ]
    routed = dot(jnp.concatenate(mix, axis=0), back_ref[...])
    for h in range(2):
        cols = slice(h * half, (h + 1) * half)
        loads[h].wait()
        out_ref[:, cols] = (routed[h * tokens : (h + 1) * tokens] + shared_ref[:, cols]).astype(BF16)
        stores[h].start()
    for store in stores:
        store.wait()
    bring.wait()


def combine(back, slots, weights, shared, cap, mixer_weight):
    tokens, width = shared.shape
    hbm = pl.BlockSpec(memory_space=pltpu.HBM)
    vmem = pl.BlockSpec(memory_space=pltpu.VMEM)
    body = lambda *refs: combine_body(cap, *refs)
    return pl.pallas_call(
        body,
        in_specs=[vmem, vmem, vmem, hbm, hbm],
        out_specs=[hbm, vmem],
        out_shape=[
            jax.ShapeDtypeStruct((tokens, width), BF16),
            pltpu.VMEM(mixer_weight.shape, BF16),
        ],
        scratch_shapes=[
            pltpu.VMEM((tokens, width), F32),
            pltpu.VMEM((tokens, width), BF16),
            pltpu.SemaphoreType.DMA((2, 2)),
            pltpu.SemaphoreType.DMA,
        ],
        compiler_params=params(20),
        cost_estimate=cost(4 * tokens * back.shape[0] * width, 2 * back.size),
        name="combine",
    )(back, slots, weights, *in_hbm(shared, mixer_weight))


def gate_rows(in_ref, forget_ref, extra_ref, bias):
    x = forget_ref[...] + bias
    log_forget = jnp.minimum(x, 0.0) - jnp.log1p(jnp.exp(-jnp.abs(x))) + extra_ref[...]
    upper = jnp.where(iota((BLK, BLK), 0) <= iota((BLK, BLK), 1), 1.0, 0.0)
    cumulative = exact_dot(log_forget, upper)
    ones = jnp.ones((BLK, BLK), F32)
    total = exact_dot(log_forget, ones)
    return in_ref[...], cumulative, total


def write_state(k_ref, v_ref, in_ref, forget_ref, extra_ref, bias_ref, out_ref):
    key_dim, length = k_ref.shape
    blocks = length // BLK
    in_gate, cumulative, total = gate_rows(in_ref, forget_ref, extra_ref, bias_ref[0])
    sums = [jnp.zeros((1, BLK), F32)]
    for j in reversed(range(1, blocks)):
        sums.insert(0, sums[0] + total[j : j + 1, :])
    after = jnp.concatenate(sums, axis=0)
    gap = after + total - cumulative + in_gate
    top = jnp.max(jnp.max(gap, axis=1, keepdims=True), axis=0, keepdims=True)
    weight = jnp.exp(gap - top)
    decay = jnp.sum(total[:, 0:1], axis=0, keepdims=True)
    acc = jnp.zeros((2 * key_dim, 2 * BLK), F32)
    ones = jnp.ones((2 * BLK, BLK), BF16)
    for j in range(blocks // 2):
        at = slice(j * 2 * BLK, (j + 1) * 2 * BLK)
        weights = jnp.concatenate([weight[2 * j : 2 * j + 1], weight[2 * j + 1 : 2 * j + 2]], axis=1)
        keys = k_ref[:, at].astype(F32) * weights
        hi, lo = split_two(keys)
        values = jnp.concatenate([v_ref[at, :], ones], axis=1)
        acc = acc + dot(jnp.concatenate([hi, lo], axis=0), values)
    state = acc[:key_dim] + acc[key_dim:]
    norm = jnp.transpose(state[:, BLK:])[0:8, :]
    norm = jnp.concatenate([norm, jnp.zeros((8, BLK - key_dim), F32)], axis=1)
    lane = iota((8, BLK), 1)
    tail = jnp.where(lane < key_dim, norm, jnp.where(lane < key_dim + 32, top, decay))
    out_ref[0:key_dim, :] = state[:, 0:BLK]
    out_ref[key_dim:, :] = tail


def merge_states(refs, keys, counted, key_dim):
    tails = [ref[key_dim : key_dim + 1, :] for ref in refs]
    tops = [t[:, key_dim : key_dim + 1] for t in tails]
    decays = [
        jnp.where(c, t[:, key_dim + 32 : key_dim + 33], 0.0) for t, c in zip(tails, counted)
    ]
    gaps = []
    for i, key in enumerate(keys):
        since = jnp.zeros((1, 1), F32)
        for j, other in enumerate(keys):
            if j != i:
                since = since + jnp.where(other > key, decays[j], 0.0)
        gaps.append(jnp.where(counted[i], tops[i] + since, NEG))
    top = gaps[0]
    for gap in gaps[1:]:
        top = jnp.maximum(top, gap)
    merged = jnp.zeros((key_dim + 8, BLK), F32)
    for ref, gap, c in zip(refs, gaps, counted):
        merged = merged + ref[...] * jnp.where(c, jnp.exp(gap - top), 0.0)
    return merged, top, sum(decays)


def as_one(scalar):
    return jnp.full((1, 1), scalar, jnp.int32)


def ring_places(place, count):
    return [as_one((place + count - k) % count) for k in range(count)]


def row_body(place_ref, *refs):
    *states, out_ref = refs
    key_dim = out_ref.shape[0] - 8
    keys = ring_places(place_ref[1], len(states))
    counted = [jnp.full((1, 1), True)] * len(states)
    merged, top, decay = merge_states(states, keys, counted, key_dim)
    lane = iota((8, BLK), 1)
    norm = merged[key_dim:, :]
    out_ref[0:key_dim, :] = merged[0:key_dim]
    out_ref[key_dim:, :] = jnp.where(
        lane < key_dim, norm, jnp.where(lane < key_dim + 32, top, decay)
    )


def row_state(place, states):
    return pl.pallas_call(
        row_body,
        in_specs=[pl.BlockSpec(memory_space=pltpu.SMEM)]
        + [pl.BlockSpec(memory_space=pltpu.VMEM)] * len(states),
        out_shape=jax.ShapeDtypeStruct(states[0].shape, F32),
        compiler_params=params(4),
        cost_estimate=cost(2**20, 2**18),
        name="row_state",
    )(place, *states)


def incoming_state(place_ref, rows, columns, key_dim):
    in_row = ring_places(place_ref[1], len(rows))
    in_column = ring_places(place_ref[0], len(columns) + 1)[1:]
    counted = [p < as_one(place_ref[1]) for p in in_row[1:]]
    counted += [p < as_one(place_ref[0]) for p in in_column]
    keys = [p + len(columns) + 1 for p in in_row[1:]] + in_column
    memory, top, _ = merge_states(rows[1:] + columns, keys, counted, key_dim)
    norm = jnp.broadcast_to(memory[key_dim : key_dim + 1, :], (BLK, BLK))
    norm = jnp.transpose(norm)[0:key_dim, :]
    return jnp.concatenate([memory[0:key_dim], norm], axis=1), top


def mixer_body(
    rows_count,
    columns_count,
    place_ref,
    bias_ref,
    q_ref,
    k_ref,
    v_ref,
    in_ref,
    forget_ref,
    extra_ref,
    gate_ref,
    gain_ref,
    *refs,
):
    key_dim, length = k_ref.shape
    blocks = length // BLK
    rows = list(refs[:rows_count])
    columns = list(refs[rows_count : rows_count + columns_count])
    *outs, out_ref = refs[rows_count + columns_count :]
    peers = len(outs)
    tokens = length // peers
    per_chunk = tokens // BLK
    in_gate, cumulative, total = gate_rows(in_ref, forget_ref, extra_ref, bias_ref[0])
    state, top = incoming_state(place_ref, rows, columns, key_dim)
    gap = total - cumulative + in_gate
    block_top = jnp.max(gap, axis=1, keepdims=True)
    weight = jnp.exp(gap - block_top)
    shifted = in_gate - cumulative
    sum_col = jnp.transpose(jnp.concatenate([cumulative] * (BLK // blocks), axis=0))
    ones = jnp.ones((BLK, BLK), BF16)
    lower = iota((BLK, BLK), 1) <= iota((BLK, BLK), 0)
    gain = gain_ref[...]
    eight = jnp.ones((8, BLK), F32)
    squares = []
    for j in range(blocks):
        at = slice(j * BLK, (j + 1) * BLK)
        keys = k_ref[:, at]
        values = jnp.concatenate([v_ref[at, :], ones], axis=1)
        query = jnp.transpose(q_ref[:, at].astype(F32) * (key_dim**-0.5)).astype(BF16)
        base = sum_col[:, j : j + 1]
        pair = jnp.where(lower, base + shifted[j : j + 1, :], -jnp.inf)
        carried = base + top
        stable = jnp.maximum(carried, jnp.max(pair, axis=1, keepdims=True))
        scores = dot(query, keys) * jnp.exp(pair - stable)
        carry = jnp.exp(carried - stable)
        score_hi, score_lo = split_two(scores)
        state_hi, state_lo = split_two(state)
        both = dot(score_hi, values) + dot(score_lo, values)
        both = both + carry * (dot(query, state_hi) + dot(query, state_lo))
        hidden = both[:, :BLK] / jnp.maximum(jnp.abs(both[:, BLK:]), jnp.exp(-stable))
        squares.append(
            exact_dot(eight, hidden * hidden, (((1,), (1,)), ((), ())))[0:1, :]
        )
        gated = hidden * gain * jax.nn.sigmoid(gate_ref[at, :].astype(F32))
        start = (j % per_chunk) * BLK
        out_ref[j // per_chunk, start : start + BLK, :] = gated.astype(BF16)
        if j + 1 < blocks:
            hi, lo = split_two(keys.astype(F32) * weight[j : j + 1, :])
            added = dot(jnp.concatenate([hi, lo], axis=0), values)
            added = added[:key_dim] + added[key_dim:]
            late = block_top[j : j + 1, :]
            early = total[j : j + 1, 0:1] + top
            top = jnp.maximum(early, late)
            state = jnp.exp(early - top) * state + jnp.exp(late - top) * added
    for c in range(peers):
        own = squares[c * per_chunk : (c + 1) * per_chunk]
        parts = [split_two(row) for row in own]
        rows = [hi.astype(F32) for hi, _ in parts] + [lo.astype(F32) for _, lo in parts]
        rows.append(jnp.zeros((16 - len(rows), BLK), F32))
        out_ref[c, tokens:, :] = jnp.concatenate(rows, axis=0).astype(BF16)
    for k in range(peers):
        outs[k][...] = out_ref[(place_ref[2] + k) % peers]


def mixer_rows(place, bias, rows, columns, queries, keys, values, in_gate, forget, extra, gate, gain, peers):
    _, length = keys.shape
    smem = pl.BlockSpec(memory_space=pltpu.SMEM)
    vmem = pl.BlockSpec(memory_space=pltpu.VMEM)
    chunk = (length // peers + 16, BLK)
    body = lambda *refs: mixer_body(len(rows), len(columns), *refs)
    return pl.pallas_call(
        body,
        in_specs=[smem, smem] + [vmem] * (8 + len(rows) + len(columns)),
        out_shape=[jax.ShapeDtypeStruct(chunk, BF16)] * peers,
        scratch_shapes=[pltpu.VMEM((peers, *chunk), BF16)],
        compiler_params=params(16),
        cost_estimate=cost(32 * length * BLK * BLK, 8 * length * BLK),
        name="mixer_rows",
    )(
        place,
        bias,
        *in_hbm(queries, keys, values, in_gate, forget, extra, gate, gain),
        *rows,
        *columns,
    )


def project_body(heads, place_ref, *refs):
    chunks = refs[:heads]
    w_ref, out_hbm, all_ref, out_ref, sems = refs[heads:]
    pieces, tokens, wide = out_ref.shape
    per_chunk = tokens // BLK
    for k in range(heads):
        all_ref[(place_ref[2] + heads - k) % heads] = chunks[k][0:tokens, :]
    tail = chunks[0][tokens:, :].astype(F32)
    for k in range(1, heads):
        tail = tail + chunks[k][tokens:, :].astype(F32)
    scales = []
    for c in range(per_chunk):
        row = tail[c : c + 1, :] + tail[per_chunk + c : per_chunk + c + 1, :]
        row = lax.rsqrt(row / (heads * BLK) + 1e-06)
        scales.append(jnp.transpose(jnp.broadcast_to(row, (BLK, BLK)))[:, 0:1])
    scale = jnp.concatenate(scales, axis=0)
    mixed = jnp.concatenate([all_ref[h] for h in range(heads)], axis=1)
    stores = []
    for p in range(pieces):
        at = slice(p * wide, (p + 1) * wide)
        out_ref[p] = (dot(mixed, w_ref[:, at]) * scale).astype(BF16)
        stores.append(pltpu.make_async_copy(out_ref.at[p], out_hbm.at[:, at], sems.at[p]))
        stores[p].start()
    for store in stores:
        store.wait()


def project(place, chunks, weight):
    heads = len(chunks)
    rows = chunks[0].shape[0]
    tokens = rows - 16
    width = weight.shape[1]
    pieces = 4
    vmem = pl.BlockSpec(memory_space=pltpu.VMEM)
    body = lambda *refs: project_body(heads, *refs)
    return pl.pallas_call(
        body,
        in_specs=[pl.BlockSpec(memory_space=pltpu.SMEM)] + [vmem] * (heads + 1),
        out_specs=pl.BlockSpec(memory_space=pltpu.HBM),
        out_shape=jax.ShapeDtypeStruct((tokens, width), BF16),
        scratch_shapes=[
            pltpu.VMEM((heads, tokens, BLK), BF16),
            pltpu.VMEM((pieces, tokens, width // pieces), BF16),
            pltpu.SemaphoreType.DMA((pieces,)),
        ],
        compiler_params=params(16),
        cost_estimate=cost(2 * tokens * weight.size, 2 * weight.size),
        name="project",
    )(place, *chunks, weight)


def exchange(x, axes):
    return lax.all_to_all(x, axes, split_axis=0, concat_axis=0, tiled=True)


def from_earlier(shards, axis):
    count = lax.axis_size(axis)
    return [
        lax.ppermute(shard, axis, [(p, (p + k) % count) for p in range(count)])
        for k, shard in enumerate(shards, 1)
    ]


def on_one(
    queries,
    head_key_rows,
    head_value_rows,
    log_input_gate,
    forget_logits,
    head_forget_bias,
    extra_log_forget,
    output_gate_logits,
    head_norm_gain,
    mixer_output_weight,
    second_batch_input,
    expert_norm_gain,
    routed_expert_index,
    routed_copy_weight,
    routed_gate_weight,
    routed_up_weight,
    routed_down_weight,
    shared_gate_weight,
    shared_up_weight,
    shared_down_weight,
):
    length = queries.shape[0]
    ep_count, tp_count = lax.axis_size(EP), lax.axis_size("tp")
    experts = ep_count * tp_count
    cap = 4

    def by_block(a):
        return a.reshape(length // BLK, BLK)

    in_gate, forget, extra = (
        by_block(log_input_gate),
        by_block(forget_logits),
        by_block(extra_log_forget),
    )
    query_rows, key_rows = queries.T, head_key_rows.T
    send, normed, slots, own = start(
        second_batch_input,
        expert_norm_gain[None, :],
        routed_expert_index.T,
        key_rows,
        head_value_rows,
        in_gate,
        forget,
        extra,
        head_forget_bias,
        cap,
        experts,
    )
    place = jnp.stack([lax.axis_index(a).astype(jnp.int32) for a in ("ep_0", "ep_1", "tp")])
    row_states = [own] + from_earlier([own] * (lax.axis_size("ep_1") - 1), "ep_1")
    row_total = row_state(place, row_states)
    column_states = from_earlier([row_total] * (lax.axis_size("ep_0") - 1), "ep_0")
    landed = exchange(send.reshape(experts, 2 * cap, -1), EP_TP)
    chunks = mixer_rows(
        place,
        head_forget_bias,
        row_states,
        column_states,
        query_rows,
        key_rows,
        head_value_rows,
        in_gate,
        forget,
        extra,
        output_gate_logits,
        head_norm_gain[None, :],
        tp_count,
    )
    shared = shared_expert(normed, shared_gate_weight, shared_up_weight, shared_down_weight)
    gathered = [chunks[0]] + from_earlier(chunks[1:], "tp")
    produced = expert_products(landed, routed_gate_weight, routed_up_weight, routed_down_weight)
    back = exchange(produced, EP_TP)
    moe_out, near_weight = combine(
        back.reshape(experts * 2 * cap, -1),
        slots,
        routed_copy_weight.T,
        shared,
        cap,
        mixer_output_weight,
    )
    mixer_first_output = project(place, gathered, near_weight)
    return (mixer_first_output, moe_out)


def solution(mesh):
    split = Mesh(mesh.devices.reshape(4, 4, mesh.shape["tp"]), ("ep_0", "ep_1", "tp"))
    return jax.shard_map(
        on_one,
        mesh=split,
        in_specs=(
            P(EP, "tp"),
            P(EP, "tp"),
            P(EP, "tp"),
            P(EP, "tp"),
            P(EP, "tp"),
            P("tp"),
            P(EP, "tp"),
            P(EP, "tp"),
            P("tp"),
            P(),
            P(EP_TP, None),
            P(),
            P(EP_TP, None),
            P(EP_TP, None),
            P(EP_TP, None, None),
            P(EP_TP, None, None),
            P(EP_TP, None, None),
            P(),
            P(),
            P(),
        ),
        out_specs=(P(EP_TP, None), P(EP_TP, None)),
        check_vma=False,
    )
```
